512 devices in a mesh: ep: 32 (over z, core), tp: 16 (over y, x).
Axes of the slice: x: 4, y: 4, z: 16, core: 2. Of those that a mesh axis runs over, the one named last changes fastest.
Arguments:
- tokens: bfloat16 [4096, 2048], P('ep'), may hold values from -6 to 6
- selected: int32 [32, 1024], P(None, 'ep'), may hold values from -1 to 127, as said below
- affinity: float32 [32, 1024], P(None, 'ep'), may hold values from 0.05 to 1
- w_gate: bfloat16 [32, 2048, 2048], P('ep', None, 'tp'), may hold values from -0.125 to 0.125
- w_up: bfloat16 [32, 2048, 2048], P('ep', None, 'tp'), may hold values from -0.125 to 0.125
- w_down: bfloat16 [32, 2048, 2048], P('ep', 'tp'), may hold values from -0.125 to 0.125
Outputs:
- combined: bfloat16 [4096, 2048], P('ep', 'tp')
The draws below stay inside these ranges and needn't reach their ends.
Inputs may be any that keep to these rules, and one draw needn't show every extreme that they name: `selected`: row e holds 32 aligned groups of 32 entries; the live entries of group j are distinct positions within the j-th block of 128 tokens, stand at the front of the group and are followed by -1; each row has 512 live entries in all, the number in a group varies, and some group of every row is full.
All inputs are finite; a program needn't handle non-finite values.
Results may differ from the reference program's by a relative error of at most 0.015.
Values may be sent and summed in bfloat16 or wider, within the bound.
No kernel may reach another device: no remote copies, remote signals or barrier semaphores. Data moves between devices by JAX's collectives and lax.ppermute only.
A program may use at most 64 MiB of HBM per device.

```python
import math
import jax
import jax.numpy as jnp
from jax import lax

D = 2048
FF = 2048
TOK_DEV = 128
EXPERTS = 32
TOKENS = 4096
PICK = 16
MOST = 32
SLOTS = 1024
N_EP = 32
N_TP = 16


def draw_selected(key, part):
    half = N_EP // 2
    block_scores = jax.random.randint(jax.random.fold_in(key, 11), (EXPERTS, N_EP), 0, 2 ** 20)
    block_order = jnp.argsort(block_scores * N_EP + jnp.arange(N_EP, dtype=jnp.int32)[None, :], axis=1, stable=True).astype(jnp.int32)
    inverse = jnp.argsort(block_order, axis=1, stable=True).astype(jnp.int32)
    shifts = jax.random.randint(jax.random.fold_in(key, 12), (EXPERTS, half), -PICK, PICK + 1)
    forced = jax.random.randint(jax.random.fold_in(key, 13), (EXPERTS,), 0, half)
    shifts = jnp.where(jnp.arange(half, dtype=jnp.int32)[None, :] == forced[:, None], PICK, shifts)
    counts_paired = jnp.concatenate([PICK + shifts, PICK - shifts], axis=1)
    counts = jnp.take_along_axis(counts_paired, inverse, axis=1)
    scores = jax.random.randint(jax.random.fold_in(key, 17), (EXPERTS, N_EP, TOK_DEV), 0, 2 ** 20)
    distinct = scores * TOK_DEV + jnp.arange(TOK_DEV, dtype=jnp.int32)[None, None, :]
    order = jnp.argsort(distinct, axis=2, stable=True).astype(jnp.int32)[:, :, :MOST]
    live = jnp.arange(MOST, dtype=jnp.int32)[None, None, :] < counts[:, :, None]
    picked = jnp.where(live, order, -1)
    return picked.reshape(EXPERTS, N_EP * MOST).astype(jnp.int32)


def shard_levels(rng, dims, shards, low, largest):
    loudness = 1.0
    for axis_at, shards_of in shards:
        steps = jax.random.uniform(jax.random.fold_in(jax.random.fold_in(rng, 6), axis_at), (shards_of,), jnp.float32, low / len(shards), largest / len(shards))
        loudness = loudness * jnp.repeat(jnp.exp(steps), dims[axis_at] // shards_of).reshape((-1,) + (1,) * (len(dims) - 1 - axis_at))
    return loudness


def normal_values(stream_key, dims, width, most, pieces=(), kind=jnp.bfloat16):
    values = jax.random.normal(stream_key, dims, jnp.float32) * width
    if len(pieces) > 0:
        values = shard_levels(stream_key, dims, pieces, -0.22, 0.18) * values
    return jnp.clip(values, min=-most, max=most).astype(kind)


def setup_inputs(seed: int = 0) -> dict:
    streams_of = jax.random.split(jax.random.key(seed), 7)
    tokens = normal_values(streams_of[0], (TOKENS, D), 1.0, 6.0, ((0, 32),))
    selected = draw_selected(jax.random.fold_in(streams_of[6], 71), 0)
    affinity = jnp.clip(jnp.exp(math.log(1.0) - 2.9957323 * jax.random.uniform(streams_of[2], (EXPERTS, SLOTS), jnp.float32) ** shard_levels(streams_of[2], (EXPERTS, SLOTS), ((1, 32),), -0.2, 0.2)), 0.05, 1.0)
    w_gate = normal_values(streams_of[3], (EXPERTS, D, FF), D ** -0.5, 0.125, ((0, 32), (2, 16)))
    w_up = normal_values(streams_of[4], (EXPERTS, D, FF), D ** -0.5, 0.125, ((0, 32), (2, 16)))
    w_down = normal_values(streams_of[5], (EXPERTS, FF, D), FF ** -0.5, 0.125, ((0, 32), (1, 16)))
    return {"tokens": tokens, "selected": selected, "affinity": affinity, "w_gate": w_gate, "w_up": w_up, "w_down": w_down}


def reference(tokens, selected, affinity, w_gate, w_up, w_down):
    offsets = (jnp.arange(SLOTS, dtype=jnp.int32) // MOST) * TOK_DEV

    def expert_step(carry, inputs):
        index_row, weight_row, gate_mat, up_mat, down_mat = inputs
        live = index_row >= 0
        position = (jnp.maximum(index_row, 0) + offsets).astype(jnp.int32)
        chosen = tokens[position]
        gate_act = jnp.dot(chosen, gate_mat, preferred_element_type=jnp.float32)
        up_act = jnp.dot(chosen, up_mat, preferred_element_type=jnp.float32)
        hidden = (jax.nn.silu(gate_act) * up_act).astype(jnp.bfloat16)
        blocks = hidden.reshape(SLOTS, N_TP, FF // N_TP).astype(jnp.float32)
        down_blocks = down_mat.reshape(N_TP, FF // N_TP, D).astype(jnp.float32)
        partial_value = jnp.einsum('ckf,kfd->kcd', blocks, down_blocks).astype(jnp.bfloat16)
        expert_out = jnp.sum(partial_value.astype(jnp.float32), axis=0).astype(jnp.bfloat16)
        scaled_weight = jnp.where(live, weight_row, jnp.zeros_like(weight_row))
        carry = carry.at[position].add(scaled_weight[:, None] * expert_out.astype(jnp.float32))
        return carry, None

    initial = jnp.zeros((TOKENS, D), jnp.float32)
    result, unused = lax.scan(expert_step, initial, (selected, affinity, w_gate, w_up, w_down))
    return result.astype(jnp.bfloat16)
```

```python
import jax
import jax.numpy as jnp
from jax import lax
from jax.experimental import pallas as pl
from jax.experimental.pallas import tpu as pltpu
from jax.sharding import Mesh
from jax.sharding import PartitionSpec as P

EP = ("ep_0", "ep_1")
BF = jnp.bfloat16
F32 = jnp.float32
EMPTY = 64.0
LIMIT = 32.0


def iota(shape, dim):
    return lax.broadcasted_iota(jnp.int32, shape, dim)


def dot(a, b):
    return jnp.dot(a, b, preferred_element_type=F32)


def one_hot(mask):
    return jnp.where(mask, 1.0, 0.0).astype(BF)


def pick_kernel(col_ref, selected_ref, affinity_ref, tokens_ref, rows_ref, mix_ref):
    experts, most = selected_ref.shape
    tok, width = tokens_ref.shape
    slots = experts * most
    sel = selected_ref[...].astype(F32).astype(BF)
    repeat = one_hot(iota((slots, experts), 0) // most == iota((slots, experts), 1))
    spread = dot(repeat, sel)
    own = iota((slots, most), 0) % most == iota((slots, most), 1)
    position = dot(jnp.where(own, spread, 0.0).astype(BF), jnp.ones((most, tok), BF))
    named = one_hot(position == iota((slots, tok), 1).astype(F32))
    rows = dot(named, tokens_ref[...])
    rows_ref[...] = jnp.where(position < 0.0, EMPTY, rows).astype(BF)
    tile = one_hot(iota((most, slots), 0) == iota((most, slots), 1) % most)
    mine = iota((experts, slots), 0) == iota((experts, slots), 1) // most

    def as_row(values):
        return jnp.sum(jnp.where(mine, dot(values, tile), 0.0), axis=0, keepdims=True)

    aff = affinity_ref[...]
    high = aff.astype(BF)
    low = (aff - high.astype(F32)).astype(BF)
    hit = as_row(sel) == iota((tok, slots), 0).astype(F32)
    mix_ref[0] = jnp.where(hit, as_row(high), 0.0).astype(BF)
    mix_ref[1] = jnp.where(hit, as_row(low), 0.0).astype(BF)


def compact_kernel(slots_ref, rows_ref):
    slots, width = slots_ref.shape
    count = rows_ref.shape[0]
    data = slots_ref[...]
    live = one_hot(data.astype(F32) < LIMIT)
    first = one_hot(iota((8, width), 1) == 0)
    live_row = lax.dot_general(first, live, (((1,), (1,)), ((), ())), preferred_element_type=F32)
    before = one_hot(iota((slots, slots), 0) < iota((slots, slots), 1))
    rank = dot(live_row.astype(BF), before)
    rank = jnp.where(live_row > 0.5, rank, -1.0)[0:1]
    take = one_hot(rank == iota((count, slots), 0).astype(F32))
    rows_ref[...] = dot(take, data).astype(BF)


def ffn_kernel(x_ref, gate_ref, up_ref, down_ref, out_ref):
    peers, rows, span = x_ref.shape
    x = jnp.concatenate([x_ref[k] for k in range(peers)], axis=1)
    gate = dot(x, gate_ref[0])
    up = dot(x, up_ref[0])
    hidden = (gate / (1.0 + jnp.exp(-gate)) * up).astype(BF)
    partial = dot(hidden, down_ref[0]).astype(BF)
    for k in range(peers):
        out_ref[k] = partial[:, k * span : (k + 1) * span]


def expand_kernel(parts_ref, slots_ref, out_ref):
    peers, count, width = parts_ref.shape
    slots = slots_ref.shape[0]
    total = parts_ref[0].astype(F32)
    for k in range(1, peers):
        total = total + parts_ref[k].astype(F32)
    live = one_hot(slots_ref[...].astype(F32) < LIMIT)
    before = one_hot(iota((slots, slots), 1) < iota((slots, slots), 0))
    rank = dot(before, live)
    rank = jnp.where(live > 0.5, rank, -1.0)
    lanes = iota((slots, width), 1).astype(F32)
    put = jnp.concatenate([one_hot(rank - k == lanes) for k in range(0, count, width)], axis=1)
    out_ref[...] = dot(put, total.astype(BF)).astype(BF)


def combine_kernel(mix_ref, rows_ref, out_ref):
    rows = rows_ref[...]
    out_ref[...] = (dot(mix_ref[0], rows) + dot(mix_ref[1], rows)).astype(BF)


def call(kernel, shapes, *args):
    return pl.pallas_call(kernel, out_shape=shapes)(*args)


def per_device(tokens, selected, affinity, w_gate, w_up, w_down):
    ep = lax.axis_size(EP)
    tp = lax.axis_size("tp")
    tok, width = tokens.shape
    experts, most = selected.shape
    slots = experts * most
    live = ep * most // 2
    span = width // tp
    col = lax.axis_index("tp").astype(jnp.int32).reshape(1)
    rows, mix = pl.pallas_call(
        pick_kernel,
        grid_spec=pltpu.PrefetchScalarGridSpec(
            num_scalar_prefetch=1,
            grid=(1,),
            in_specs=[
                pl.BlockSpec((experts, most), lambda i, c: (0, 0)),
                pl.BlockSpec((experts, most), lambda i, c: (0, 0)),
                pl.BlockSpec((tok, span), lambda i, c: (0, c[0])),
            ],
            out_specs=[
                pl.BlockSpec((slots, span), lambda i, c: (0, 0)),
                pl.BlockSpec((2, tok, slots), lambda i, c: (0, 0, 0)),
            ],
        ),
        out_shape=[
            jax.ShapeDtypeStruct((slots, span), BF),
            jax.ShapeDtypeStruct((2, tok, slots), BF),
        ],
    )(col, selected, affinity, tokens)
    arrived = lax.all_to_all(rows.reshape(experts, most, span), EP, 0, 0, tiled=True)
    arrived = arrived.reshape(ep * most, span)
    packed = call(compact_kernel, jax.ShapeDtypeStruct((live, span), BF), arrived)
    chosen = lax.all_to_all(
        jnp.broadcast_to(packed[None], (tp, live, span)), "tp", 0, 0, tiled=True
    )
    steps = 2
    part = live // steps
    partial = pl.pallas_call(
        ffn_kernel,
        grid=(steps,),
        in_specs=[
            pl.BlockSpec((tp, part, span), lambda i: (0, i, 0)),
            pl.BlockSpec(w_gate.shape, lambda i: (0, 0, 0)),
            pl.BlockSpec(w_up.shape, lambda i: (0, 0, 0)),
            pl.BlockSpec(w_down.shape, lambda i: (0, 0, 0)),
        ],
        out_specs=pl.BlockSpec((tp, part, span), lambda i: (0, i, 0)),
        out_shape=jax.ShapeDtypeStruct((tp, live, span), BF),
    )(chosen, w_gate, w_up, w_down)
    summands = lax.all_to_all(partial, "tp", 0, 0, tiled=True)
    result = call(
        expand_kernel, jax.ShapeDtypeStruct((ep * most, span), BF), summands, arrived
    )
    returned = lax.all_to_all(result.reshape(ep, most, span), EP, 0, 0, tiled=True)
    return call(
        combine_kernel,
        jax.ShapeDtypeStruct((tok, span), BF),
        mix,
        returned.reshape(slots, span),
    )


def solution(mesh):
    torus = Mesh(mesh.devices.reshape(16, 2, mesh.shape["tp"]), ("ep_0", "ep_1", "tp"))
    in_specs = (
        P(EP, None),
        P(None, EP),
        P(None, EP),
        P(EP, None, "tp"),
        P(EP, None, "tp"),
        P(EP, "tp", None),
    )
    return jax.shard_map(
        per_device, mesh=torus, in_specs=in_specs, out_specs=P(EP, "tp"), check_vma=False
    )
```

```python
import jax
import jax.numpy as jnp
from jax import lax
from jax.experimental import pallas as pl
from jax.experimental.pallas import tpu as pltpu
from jax.sharding import Mesh
from jax.sharding import PartitionSpec as P

EP = ("z", "c")
TP = ("g", "yy", "x")
TEAM = ("c", "yy", "x")
BF = jnp.bfloat16
F32 = jnp.float32
EMPTY = 64.0
LIMIT = 32.0
TRADE = [(0, 0), (1, 1), (6, 6), (7, 7), (4, 3), (3, 4), (5, 2), (2, 5)]
PAIR = [(0, 3), (3, 0), (1, 2), (2, 1)]
CORES = [(0, 1), (1, 0)]


def iota(shape, dim):
    return lax.broadcasted_iota(jnp.int32, shape, dim)


def dot(a, b):
    return jnp.dot(a, b, preferred_element_type=F32)


def one_hot(mask):
    return jnp.where(mask, 1.0, 0.0).astype(BF)


def pack_kernel(gate_ref, up_ref, down_ref, out_ref):
    width = gate_ref.shape[1]
    span = gate_ref.shape[2]
    out_ref[:width] = gate_ref[0]
    out_ref[width : 2 * width] = up_ref[0]
    for k in range(width // span):
        at = 2 * width + k * span
        out_ref[at : at + span] = down_ref[0, :, k * span : (k + 1) * span]


def pick_kernel(place_ref, selected_ref, affinity_ref, first_ref, second_ref, rows_ref, mix_ref):
    g = place_ref[2]
    experts, most = selected_ref.shape
    tok, width = first_ref.shape
    here = experts // 2
    slots = here * most
    sel = selected_ref[...].astype(F32).astype(BF)
    repeat = one_hot(2 * (iota((slots, experts), 0) // most) + g == iota((slots, experts), 1))
    own = iota((slots, most), 0) % most == iota((slots, most), 1)
    spread = jnp.where(own, dot(repeat, sel), 0.0).astype(BF)
    position = dot(spread, jnp.ones((most, tok), BF))
    named = one_hot(position == iota((slots, tok), 1).astype(F32))
    for c, ref in enumerate((first_ref, second_ref)):
        rows = jnp.where(position < 0.0, EMPTY, dot(named, ref[...])).astype(BF)
        rows_ref[:, c] = rows.reshape(here, most, width)
    tile = one_hot(iota((most, slots), 0) == iota((most, slots), 1) % most)
    mine = iota((experts, slots), 0) == 2 * (iota((experts, slots), 1) // most) + g

    def as_row(values):
        return jnp.sum(jnp.where(mine, dot(values, tile), 0.0), axis=0, keepdims=True)

    aff = affinity_ref[...]
    high = aff.astype(BF)
    low = (aff - high.astype(F32)).astype(BF)
    hit = as_row(sel) == iota((tok, slots), 0).astype(F32)
    mix_ref[0] = jnp.where(hit, as_row(high), 0.0).astype(BF)
    mix_ref[1] = jnp.where(hit, as_row(low), 0.0).astype(BF)


def compact_kernel(slots_ref, rows_ref):
    blocks, most, width = slots_ref.shape
    cores, peers, part, _ = rows_ref.shape
    slots = blocks * most
    count = cores * part
    data = slots_ref[...].reshape(slots, width)
    live = one_hot(data.astype(F32) < LIMIT)
    first = one_hot(iota((8, width), 1) == 0)
    live_row = lax.dot_general(first, live, (((1,), (1,)), ((), ())), preferred_element_type=F32)
    in_block = one_hot(iota((slots, blocks), 0) // most == iota((slots, blocks), 1))
    before = one_hot(iota((blocks, slots), 0) < iota((blocks, slots), 1) // most)
    counts = dot(live_row.astype(BF), in_block)
    rank = dot(counts.astype(BF), before) + (iota((8, slots), 1) % most).astype(F32)
    rank = jnp.where(live_row > 0.5, rank, -1.0)[0:1]
    take = one_hot(rank == iota((count, slots), 0).astype(F32))
    rows = dot(take, data).astype(BF)
    for c in range(cores):
        for k in range(peers):
            rows_ref[c, k] = rows[c * part : (c + 1) * part]


def seat(block, g):
    y = block // 4
    yy = (0, 1, 1, 0)[y]
    return (y // 2) * 8 + 4 * (yy + g - 2 * yy * g) + block % 4


def ffn_kernel(place_ref, x_ref, mine_ref, other_ref, out_ref):
    g = place_ref[2]
    peers, rows, span = x_ref.shape
    width = peers * span
    pair = (mine_ref, other_ref)
    x = jnp.concatenate([x_ref[seat(k, g)] for k in range(peers)], axis=1)
    gate = dot(x, jnp.concatenate([w[:width] for w in pair], axis=1))
    up = dot(x, jnp.concatenate([w[width : 2 * width] for w in pair], axis=1))
    hidden = (gate / (1.0 + jnp.exp(-gate)) * up).astype(BF)
    for k in range(0, peers, 2):
        at = 2 * width + k * span
        tiles = [
            jnp.concatenate([w[at + j * span : at + (j + 1) * span] for w in pair], axis=0)
            for j in range(2)
        ]
        partial = dot(hidden, jnp.concatenate(tiles, axis=1)).astype(BF)
        for j in range(2):
            out_ref[seat(k + j, g)] = partial[:, j * span : (j + 1) * span]


def expand_kernel(parts_ref, slots_ref, out_ref):
    cores, peers, part, width = parts_ref.shape
    blocks, most, _ = slots_ref.shape
    slots = blocks * most
    halves = []
    for c in range(cores):
        total = parts_ref[c, 0].astype(F32)
        for k in range(1, peers):
            total = total + parts_ref[c, k].astype(F32)
        halves.append(total.astype(BF))
    live = one_hot(slots_ref[...].reshape(slots, width).astype(F32) < LIMIT)
    in_block = one_hot(iota((blocks, slots), 0) == iota((blocks, slots), 1) // most)
    before = one_hot(iota((slots, blocks), 1) < iota((slots, blocks), 0) // most)
    counts = dot(in_block, live).astype(BF)
    rank = dot(before, counts) + (iota((slots, width), 0) % most).astype(F32)
    rank = jnp.where(live > 0.5, rank, -1.0)
    lanes = iota((slots, width), 1).astype(F32)
    put = [one_hot(rank - k == lanes) for k in range(0, cores * part, width)]
    rows = dot(jnp.concatenate(put, axis=1), jnp.concatenate(halves, axis=0)).astype(BF)
    out_ref[...] = rows.reshape(blocks, most, width)


def combine_kernel(place_ref, mix_ref, rows_ref, keep_ref, send_ref):
    here, cores, most, width = rows_ref.shape
    both = [rows_ref[:, c].reshape(here * most, width) for c in range(cores)]
    both = jnp.concatenate(both, axis=1)
    total = dot(mix_ref[0], both) + dot(mix_ref[1], both)
    mine = place_ref[2] == 0
    keep_ref[...] = jnp.where(mine, total[:, :width], total[:, width:])
    send_ref[...] = jnp.where(mine, total[:, width:], total[:, :width])


def whole(shape):
    return pl.BlockSpec(shape, lambda i, place: (0,) * len(shape))


def placed_call(kernel, place, outs, *args, specs=None):
    specs = specs or [whole(a.shape) for a in args]
    return pl.pallas_call(
        kernel,
        grid_spec=pltpu.PrefetchScalarGridSpec(
            num_scalar_prefetch=1,
            grid=(1,),
            in_specs=specs,
            out_specs=jax.tree.map(lambda o: whole(o.shape), outs),
        ),
        out_shape=outs,
    )(place, *args)


def array(shape, dtype=BF):
    return jax.ShapeDtypeStruct(shape, dtype)


def per_device(tokens, selected, affinity, w_gate, w_up, w_down):
    ep = lax.axis_size(EP)
    layers = lax.axis_size("z")
    team = lax.axis_size(TEAM)
    tok, width = tokens.shape
    experts, most = selected.shape
    span = width // team
    part = ep * most // 4
    g = lax.axis_index("g")
    y = 2 * g + lax.axis_index("yy")
    x = lax.axis_index("x")
    place = jnp.stack([4 * jnp.minimum(y, 3 - y) + x, 4 * jnp.maximum(y, 3 - y) + x, g])
    place = place.astype(jnp.int32)
    packed = pl.pallas_call(pack_kernel, out_shape=array((3 * width, span)))(
        w_gate, w_up, w_down
    )
    mine = lax.ppermute(packed, ("c", "g", "yy"), TRADE)
    other = lax.ppermute(mine, "c", CORES)
    rows, mix = placed_call(
        pick_kernel,
        place,
        [array((layers, 2, most, span)), array((2, tok, layers * most))],
        selected,
        affinity,
        tokens,
        tokens,
        specs=[
            whole(selected.shape),
            whole(affinity.shape),
            pl.BlockSpec((tok, span), lambda i, place: (0, place[0])),
            pl.BlockSpec((tok, span), lambda i, place: (0, place[1])),
        ],
    )
    arrived = lax.all_to_all(rows.reshape(ep, most, span), EP, 0, 0, tiled=True)
    copies = pl.pallas_call(compact_kernel, out_shape=array((2, team // 2, part, span)))(arrived)
    chosen = lax.all_to_all(copies.reshape(team, part, span), TEAM, 0, 0, tiled=True)
    partial = placed_call(ffn_kernel, place, array((team, part, span)), chosen, mine, other)
    summands = lax.all_to_all(partial, TEAM, 0, 0, tiled=True)
    result = pl.pallas_call(expand_kernel, out_shape=array((ep, most, span)))(
        summands.reshape(2, team // 2, part, span), arrived
    )
    returned = lax.all_to_all(result, EP, 0, 0, tiled=True)
    keep, send = placed_call(
        combine_kernel,
        place,
        [array((tok, span), F32), array((tok, span), F32)],
        mix,
        returned.reshape(layers, 2, most, span),
    )
    return (keep + lax.ppermute(send, ("g", "yy"), PAIR)).astype(BF)


def solution(mesh):
    torus = Mesh(mesh.devices.reshape(16, 2, 2, 2, 4), ("z", "c", "g", "yy", "x"))
    in_specs = (
        P(EP, None),
        P(None, EP),
        P(None, EP),
        P(EP, None, TP),
        P(EP, None, TP),
        P(EP, TP, None),
    )
    return jax.shard_map(
        per_device, mesh=torus, in_specs=in_specs, out_specs=P(EP, TP), check_vma=False
    )
```

```python
import jax
import jax.numpy as jnp
from jax import lax
from jax.experimental import pallas as pl
from jax.experimental.pallas import tpu as pltpu
from jax.sharding import Mesh
from jax.sharding import PartitionSpec as P

EP = ("z", "c")
TP = ("g", "yy", "x")
TEAM = ("c", "yy", "x")
BF = jnp.bfloat16
F32 = jnp.float32
EMPTY = 64.0
LIMIT = 32.0
TRADE = [(0, 0), (1, 1), (6, 6), (7, 7), (4, 3), (3, 4), (5, 2), (2, 5)]
PAIR = [(0, 3), (3, 0), (1, 2), (2, 1)]
CORES = [(0, 1), (1, 0)]


def iota(shape, dim):
    return lax.broadcasted_iota(jnp.int32, shape, dim)


def dot(a, b):
    return jnp.dot(a, b, preferred_element_type=F32)


def one_hot(mask):
    return jnp.where(mask, 1.0, 0.0).astype(BF)


def whereabouts(place_ref):
    place = place_ref[0]
    return place // 8, place // 4, place % 4


def pack_kernel(gate_ref, up_ref, down_ref, out_ref, sems):
    _, width, span = gate_ref.shape
    copies = [(gate_ref.at[0], out_ref.at[:width]), (up_ref.at[0], out_ref.at[width : 2 * width])]
    for k in range(width // span):
        at = 2 * width + k * span
        copies.append((down_ref.at[0, :, k * span : (k + 1) * span], out_ref.at[at : at + span]))
    copies = [pltpu.make_async_copy(*c, sems.at[k]) for k, c in enumerate(copies)]
    for copy in copies:
        copy.start()
    for copy in copies:
        copy.wait()


def pick_kernel(place_ref, selected_ref, affinity_ref, tokens_ref, rows_ref, mix_ref, tile_ref, sems):
    g, y, x = whereabouts(place_ref)
    experts, most = selected_ref.shape
    _, tok, width = tile_ref.shape
    copies = []
    for c in range(2):
        block = 4 * ((jnp.minimum, jnp.maximum)[c](y, 3 - y)) + x
        at = pl.multiple_of(block * width, width)
        copies.append(
            pltpu.make_async_copy(tokens_ref.at[:, pl.ds(at, width)], tile_ref.at[c], sems.at[c])
        )
        copies[c].start()
    here = experts // 2
    slots = here * most
    sel = selected_ref[...].astype(F32).astype(BF)
    repeat = one_hot(2 * (iota((slots, experts), 0) // most) + g == iota((slots, experts), 1))
    own = iota((slots, most), 0) % most == iota((slots, most), 1)
    spread = jnp.where(own, dot(repeat, sel), 0.0).astype(BF)
    position = dot(spread, jnp.ones((most, tok), BF))
    named = one_hot(position == iota((slots, tok), 1).astype(F32))
    tile = one_hot(iota((most, slots), 0) == iota((most, slots), 1) % most)
    mine = iota((experts, slots), 0) == 2 * (iota((experts, slots), 1) // most) + g

    def as_row(values):
        return jnp.sum(jnp.where(mine, dot(values, tile), 0.0), axis=0, keepdims=True)

    aff = affinity_ref[...]
    high = aff.astype(BF)
    low = (aff - high.astype(F32)).astype(BF)
    hit = as_row(sel) == iota((tok, slots), 0).astype(F32)
    mix_ref[0] = jnp.where(hit, as_row(high), 0.0).astype(BF)
    mix_ref[1] = jnp.where(hit, as_row(low), 0.0).astype(BF)
    for c in range(2):
        copies[c].wait()
        rows = jnp.where(position < 0.0, EMPTY, dot(named, tile_ref[c])).astype(BF)
        rows_ref[:, c] = rows.reshape(here, most, width)


def compact_kernel(slots_ref, rows_ref):
    blocks, most, width = slots_ref.shape
    cores, peers, part, _ = rows_ref.shape
    slots = blocks * most
    count = cores * part
    data = slots_ref[...].reshape(slots, width)
    live = one_hot(data.astype(F32) < LIMIT)
    first = one_hot(iota((8, width), 1) == 0)
    live_row = lax.dot_general(first, live, (((1,), (1,)), ((), ())), preferred_element_type=F32)
    in_block = one_hot(iota((slots, blocks), 0) // most == iota((slots, blocks), 1))
    before = one_hot(iota((blocks, slots), 0) < iota((blocks, slots), 1) // most)
    counts = dot(live_row.astype(BF), in_block)
    rank = dot(counts.astype(BF), before) + (iota((8, slots), 1) % most).astype(F32)
    rank = jnp.where(live_row > 0.5, rank, -1.0)[0:1]
    take = one_hot(rank == iota((count, slots), 0).astype(F32))
    rows = dot(take, data).astype(BF)
    for c in range(cores):
        for k in range(peers):
            rows_ref[c, k] = rows[c * part : (c + 1) * part]


def seat(block, g):
    y = block // 4
    yy = (0, 1, 1, 0)[y]
    return (y // 2) * 8 + 4 * (yy + g - 2 * yy * g) + block % 4


def ffn_kernel(place_ref, x_ref, mine_ref, other_ref, out_ref):
    g, _, _ = whereabouts(place_ref)
    peers, rows, span = x_ref.shape
    width = peers * span
    pair = (mine_ref, other_ref)
    x = jnp.concatenate([x_ref[seat(k, g)] for k in range(peers)], axis=1)
    gate = dot(x, jnp.concatenate([w[:width] for w in pair], axis=1))
    up = dot(x, jnp.concatenate([w[width : 2 * width] for w in pair], axis=1))
    hidden = (gate / (1.0 + jnp.exp(-gate)) * up).astype(BF)
    for k in range(0, peers, 2):
        at = 2 * width + k * span
        tiles = [
            jnp.concatenate([w[at + j * span : at + (j + 1) * span] for w in pair], axis=0)
            for j in range(2)
        ]
        partial = dot(hidden, jnp.concatenate(tiles, axis=1)).astype(BF)
        for j in range(2):
            out_ref[seat(k + j, g)] = partial[:, j * span : (j + 1) * span]


def expand_kernel(parts_ref, slots_ref, out_ref):
    cores, peers, part, width = parts_ref.shape
    blocks, most, _ = slots_ref.shape
    slots = blocks * most
    halves = []
    for c in range(cores):
        total = parts_ref[c, 0].astype(F32)
        for k in range(1, peers):
            total = total + parts_ref[c, k].astype(F32)
        halves.append(total.astype(BF))
    live = one_hot(slots_ref[...].reshape(slots, width).astype(F32) < LIMIT)
    in_block = one_hot(iota((blocks, slots), 0) == iota((blocks, slots), 1) // most)
    before = one_hot(iota((slots, blocks), 1) < iota((slots, blocks), 0) // most)
    counts = dot(in_block, live).astype(BF)
    rank = dot(before, counts) + (iota((slots, width), 0) % most).astype(F32)
    rank = jnp.where(live > 0.5, rank, -1.0)
    lanes = iota((slots, width), 1).astype(F32)
    put = [one_hot(rank - k == lanes) for k in range(0, cores * part, width)]
    rows = dot(jnp.concatenate(put, axis=1), jnp.concatenate(halves, axis=0)).astype(BF)
    out_ref[...] = rows.reshape(blocks, most, width)


def combine_kernel(place_ref, mix_ref, rows_ref, keep_ref, send_ref):
    here, cores, most, width = rows_ref.shape
    both = [rows_ref[:, c].reshape(here * most, width) for c in range(cores)]
    both = jnp.concatenate(both, axis=1)
    total = dot(mix_ref[0], both) + dot(mix_ref[1], both)
    mine = whereabouts(place_ref)[0] == 0
    keep_ref[...] = jnp.where(mine, total[:, :width], total[:, width:])
    send_ref[...] = jnp.where(mine, total[:, width:], total[:, :width]).astype(BF)


def local_call(kernel, outs, *args, place=None, params=(), hbm=(), scratch=()):
    vmem = pl.BlockSpec(memory_space=pltpu.VMEM)
    specs = [pl.BlockSpec()] * len(params) + [vmem] * len(args)
    specs += [pl.BlockSpec(memory_space=pltpu.HBM)] * len(hbm)
    args = [pltpu.with_memory_space_constraint(a, pltpu.VMEM) for a in args]
    args = [*params, *args, *(pltpu.with_memory_space_constraint(a, pltpu.HBM) for a in hbm)]
    if place is not None:
        specs = [pl.BlockSpec(memory_space=pltpu.SMEM)] + specs
        args = [place] + args
    return pl.pallas_call(
        kernel,
        in_specs=specs,
        out_specs=jax.tree.map(
            lambda o: pl.BlockSpec() if isinstance(o, jax.ShapeDtypeStruct) else vmem, outs
        ),
        out_shape=outs,
        scratch_shapes=scratch,
        compiler_params=pltpu.CompilerParams(vmem_limit_bytes=24 * 2**20),
    )(*args)


def array(shape, dtype=BF):
    return pltpu.VMEM(shape, dtype)


def per_device(tokens, selected, affinity, w_gate, w_up, w_down):
    ep = lax.axis_size(EP)
    layers = lax.axis_size("z")
    team = lax.axis_size(TEAM)
    tok, width = tokens.shape
    experts, most = selected.shape
    span = width // team
    part = ep * most // 4
    place = lax.axis_index(TP).astype(jnp.int32).reshape(1)
    packed = local_call(
        pack_kernel,
        array((3 * width, span)),
        hbm=(w_gate, w_up, w_down),
        scratch=[pltpu.SemaphoreType.DMA((2 + team,))],
    )
    mine = lax.ppermute(packed, ("c", "g", "yy"), TRADE)
    other = lax.ppermute(mine, "c", CORES)
    rows, mix = local_call(
        pick_kernel,
        [
            jax.ShapeDtypeStruct((layers, 2, most, span), BF),
            jax.ShapeDtypeStruct((2, tok, layers * most), BF),
        ],
        place=place,
        params=(selected, affinity),
        hbm=(tokens,),
        scratch=[pltpu.VMEM((2, tok, span), BF), pltpu.SemaphoreType.DMA((2,))],
    )
    arrived = lax.all_to_all(rows.reshape(ep, most, span), EP, 0, 0, tiled=True)
    copies = local_call(compact_kernel, array((2, team // 2, part, span)), arrived)
    chosen = lax.all_to_all(copies.reshape(team, part, span), TEAM, 0, 0, tiled=True)
    partial = local_call(ffn_kernel, array((team, part, span)), chosen, mine, other, place=place)
    summands = lax.all_to_all(partial, TEAM, 0, 0, tiled=True)
    result = local_call(
        expand_kernel,
        array((ep, most, span)),
        summands.reshape(2, team // 2, part, span),
        arrived,
    )
    returned = lax.all_to_all(result, EP, 0, 0, tiled=True)
    keep, send = local_call(
        combine_kernel,
        [array((tok, span), F32), array((tok, span))],
        mix,
        returned.reshape(layers, 2, most, span),
        place=place,
    )
    return (keep + lax.ppermute(send, ("g", "yy"), PAIR).astype(F32)).astype(BF)


def solution(mesh):
    torus = Mesh(mesh.devices.reshape(16, 2, 2, 2, 4), ("z", "c", "g", "yy", "x"))
    in_specs = (
        P(EP, None),
        P(None, EP),
        P(None, EP),
        P(EP, None, TP),
        P(EP, None, TP),
        P(EP, TP, None),
    )
    return jax.shard_map(
        per_device, mesh=torus, in_specs=in_specs, out_specs=P(EP, TP), check_vma=False
    )
```

```python
import jax
import jax.numpy as jnp
from jax import lax
from jax.experimental import pallas as pl
from jax.experimental.pallas import tpu as pltpu
from jax.sharding import Mesh
from jax.sharding import PartitionSpec as P

EP = ("z", "c")
TP = ("g", "yy", "x")
TEAM = ("c", "yy", "x")
BF = jnp.bfloat16
F32 = jnp.float32
EMPTY = 64.0
LIMIT = 32.0
TRADE = [(0, 0), (1, 1), (6, 6), (7, 7), (4, 3), (3, 4), (5, 2), (2, 5)]
PAIR = [(0, 3), (3, 0), (1, 2), (2, 1)]
ACROSS = [(0, 1), (1, 0), (2, 3), (3, 2), (4, 7), (7, 4), (5, 6), (6, 5)]
CORES = [(0, 1), (1, 0)]


def iota(shape, dim):
    return lax.broadcasted_iota(jnp.int32, shape, dim)


def dot(a, b):
    return jnp.dot(a, b, preferred_element_type=F32)


def one_hot(mask):
    return jnp.where(mask, 1.0, 0.0).astype(BF)


def whereabouts(place_ref):
    place = place_ref[0]
    return place // 8, place // 4, place % 4


def pack_kernel(gate_ref, up_ref, down_ref, out_ref, sems):
    _, width, span = gate_ref.shape
    copies = [(gate_ref.at[0], out_ref.at[:width]), (up_ref.at[0], out_ref.at[width : 2 * width])]
    for k in range(width // span):
        at = 2 * width + k * span
        copies.append((down_ref.at[0, :, k * span : (k + 1) * span], out_ref.at[at : at + span]))
    copies = [pltpu.make_async_copy(*c, sems.at[k]) for k, c in enumerate(copies)]
    for copy in copies:
        copy.start()
    for copy in copies:
        copy.wait()


def pick_kernel(place_ref, selected_ref, tokens_ref, rows_ref, tile_ref, out_ref, sems):
    g, y, x = whereabouts(place_ref)
    experts, most = selected_ref.shape
    _, tok, width = tile_ref.shape
    loads = []
    for c in range(2):
        block = 4 * ((jnp.minimum, jnp.maximum)[c](y, 3 - y)) + x
        at = pl.multiple_of(block * width, width)
        loads.append(
            pltpu.make_async_copy(tokens_ref.at[:, pl.ds(at, width)], tile_ref.at[c], sems.at[c])
        )
        loads[c].start()
    here = experts // 2
    slots = here * most
    sel = selected_ref[...].astype(F32).astype(BF)
    repeat = one_hot(2 * (iota((slots, experts), 0) // most) + g == iota((slots, experts), 1))
    own = iota((slots, most), 0) % most == iota((slots, most), 1)
    spread = jnp.where(own, dot(repeat, sel), 0.0).astype(BF)
    position = dot(spread, jnp.ones((most, tok), BF))
    named = one_hot(position == iota((slots, tok), 1).astype(F32))
    stores = []
    for c in range(2):
        loads[c].wait()
        rows = jnp.where(position < 0.0, EMPTY, dot(named, tile_ref[c])).astype(BF)
        out_ref[c] = rows.reshape(here, most, width)
        stores.append(pltpu.make_async_copy(out_ref.at[c], rows_ref.at[:, c], sems.at[2 + c]))
        stores[c].start()
    for store in stores:
        store.wait()


def mix_kernel(place_ref, selected_ref, affinity_ref, mix_ref):
    g, _, _ = whereabouts(place_ref)
    experts, most = selected_ref.shape
    _, tok, slots = mix_ref.shape
    sel = selected_ref[...].astype(F32).astype(BF)
    tile = one_hot(iota((most, slots), 0) == iota((most, slots), 1) % most)
    mine = iota((experts, slots), 0) == 2 * (iota((experts, slots), 1) // most) + g

    def as_row(values):
        return jnp.sum(jnp.where(mine, dot(values, tile), 0.0), axis=0, keepdims=True)

    aff = affinity_ref[...]
    high = aff.astype(BF)
    low = (aff - high.astype(F32)).astype(BF)
    hit = as_row(sel) == iota((tok, slots), 0).astype(F32)
    mix_ref[0] = jnp.where(hit, as_row(high), 0.0).astype(BF)
    mix_ref[1] = jnp.where(hit, as_row(low), 0.0).astype(BF)


def compact_kernel(slots_ref, rows_ref):
    blocks, most, width = slots_ref.shape
    cores, lines, peers, part, _ = rows_ref.shape
    slots = blocks * most
    count = 2 * cores * part
    data = slots_ref[...].reshape(slots, width)
    live = one_hot(data.astype(F32) < LIMIT)
    first = one_hot(iota((8, width), 1) == 0)
    live_row = lax.dot_general(first, live, (((1,), (1,)), ((), ())), preferred_element_type=F32)
    in_block = one_hot(iota((slots, blocks), 0) // most == iota((slots, blocks), 1))
    before = one_hot(iota((blocks, slots), 0) < iota((blocks, slots), 1) // most)
    counts = dot(live_row.astype(BF), in_block)
    rank = dot(counts.astype(BF), before) + (iota((8, slots), 1) % most).astype(F32)
    rank = jnp.where(live_row > 0.5, rank, -1.0)[0:1]
    take = one_hot(rank == iota((count, slots), 0).astype(F32))
    rows = dot(take, data).astype(BF)
    for c in range(cores):
        for k in range(lines):
            for x in range(peers):
                at = (2 * (x % 2) + c) * part
                rows_ref[c, k, x] = rows[at : at + part]


def seat(block, g):
    y = block // 4
    yy = (0, 1, 1, 0)[y]
    return (y // 2) * 8 + 4 * (yy + g - 2 * yy * g) + block % 4


def ffn_kernel(place_ref, x_ref, *refs):
    *weights, out_ref = refs
    g, _, _ = whereabouts(place_ref)
    peers, _, span = x_ref.shape
    width = peers * span
    x = jnp.concatenate([x_ref[seat(k, g)] for k in range(peers)], axis=1)
    gate = dot(x, jnp.concatenate([w[:width] for w in weights], axis=1))
    up = dot(x, jnp.concatenate([w[width : 2 * width] for w in weights], axis=1))
    hidden = (gate / (1.0 + jnp.exp(-gate)) * up).astype(BF)
    for k in range(0, peers, 2):
        at = 2 * width + k * span
        tiles = [
            jnp.concatenate([w[at + j * span : at + (j + 1) * span] for w in weights], axis=0)
            for j in range(2)
        ]
        partial = dot(hidden, jnp.concatenate(tiles, axis=1)).astype(BF)
        for j in range(2):
            out_ref[seat(k + j, g)] = partial[:, j * span : (j + 1) * span]


def expand_kernel(parts_ref, slots_ref, out_ref):
    cores, lines, _, part, width = parts_ref.shape
    blocks, most, _ = slots_ref.shape
    slots = blocks * most
    quarters = []
    for x in range(2):
        for c in range(cores):
            total = parts_ref[c, 0, x].astype(F32)
            for k in range(1, 2 * lines):
                total = total + parts_ref[c, k % lines, x + 2 * (k // lines)].astype(F32)
            quarters.append(total.astype(BF))
    live = one_hot(slots_ref[...].reshape(slots, width).astype(F32) < LIMIT)
    in_block = one_hot(iota((blocks, slots), 0) == iota((blocks, slots), 1) // most)
    before = one_hot(iota((slots, blocks), 1) < iota((slots, blocks), 0) // most)
    counts = dot(in_block, live).astype(BF)
    rank = dot(before, counts) + (iota((slots, width), 0) % most).astype(F32)
    rank = jnp.where(live > 0.5, rank, -1.0)
    lanes = iota((slots, width), 1).astype(F32)
    put = [one_hot(rank - k == lanes) for k in range(0, 2 * cores * part, width)]
    rows = dot(jnp.concatenate(put, axis=1), jnp.concatenate(quarters, axis=0)).astype(BF)
    out_ref[...] = rows.reshape(blocks, most, width)


def combine_kernel(place_ref, mix_ref, rows_ref, keep_ref, send_ref):
    here, cores, most, width = rows_ref.shape
    both = [rows_ref[:, c].reshape(here * most, width) for c in range(cores)]
    both = jnp.concatenate(both, axis=1)
    total = dot(mix_ref[0], both) + dot(mix_ref[1], both)
    mine = whereabouts(place_ref)[0] == 0
    keep_ref[...] = jnp.where(mine, total[:, :width], total[:, width:])
    send_ref[...] = jnp.where(mine, total[:, width:], total[:, :width]).astype(BF)


def local_call(kernel, outs, *args, place=None, params=(), hbm=(), scratch=()):
    vmem = pl.BlockSpec(memory_space=pltpu.VMEM)
    specs = [pl.BlockSpec()] * len(params) + [vmem] * len(args)
    specs += [pl.BlockSpec(memory_space=pltpu.HBM)] * len(hbm)
    args = [pltpu.with_memory_space_constraint(a, pltpu.VMEM) for a in args]
    args = [*params, *args, *(pltpu.with_memory_space_constraint(a, pltpu.HBM) for a in hbm)]
    if place is not None:
        specs = [pl.BlockSpec(memory_space=pltpu.SMEM)] + specs
        args = [place] + args
    return pl.pallas_call(
        kernel,
        in_specs=specs,
        out_specs=jax.tree.map(lambda o: pl.BlockSpec(memory_space=o.memory_space), outs),
        out_shape=outs,
        scratch_shapes=scratch,
        compiler_params=pltpu.CompilerParams(vmem_limit_bytes=24 * 2**20),
    )(*args)


def array(shape, dtype=BF):
    return pltpu.VMEM(shape, dtype)


def per_device(tokens, selected, affinity, w_gate, w_up, w_down):
    ep = lax.axis_size(EP)
    layers = lax.axis_size("z")
    team = lax.axis_size(TEAM)
    tok, width = tokens.shape
    _, most = selected.shape
    span = width // team
    part = ep * most // 8
    lines = lax.axis_size("yy")
    peers = lax.axis_size("x")
    place = lax.axis_index(TP).astype(jnp.int32).reshape(1)
    packed = local_call(
        pack_kernel,
        array((3 * width, span)),
        hbm=(w_gate, w_up, w_down),
        scratch=[pltpu.SemaphoreType.DMA((2 + team,))],
    )
    mine = lax.ppermute(packed, ("c", "g", "yy"), TRADE)
    rows = local_call(
        pick_kernel,
        pltpu.HBM((layers, 2, most, span), BF),
        place=place,
        params=(selected,),
        hbm=(tokens,),
        scratch=[
            pltpu.VMEM((2, tok, span), BF),
            pltpu.VMEM((2, layers, most, span), BF),
            pltpu.SemaphoreType.DMA((4,)),
        ],
    )
    arrived = lax.all_to_all(rows.reshape(ep, most, span), EP, 0, 0, tiled=True)
    mix = local_call(
        mix_kernel,
        array((2, tok, layers * most)),
        place=place,
        params=(selected, affinity),
    )
    third = lax.ppermute(mine, ("c", "x"), ACROSS)
    other = lax.ppermute(mine, "c", CORES)
    copies = local_call(compact_kernel, array((2, lines, peers, part, span)), arrived)
    chosen = lax.all_to_all(copies.reshape(team, part, span), TEAM, 0, 0, tiled=True)
    fourth = lax.ppermute(third, "c", CORES)
    partial = local_call(
        ffn_kernel,
        array((team, part, span)),
        chosen,
        mine,
        other,
        third,
        fourth,
        place=place,
    )
    summands = lax.all_to_all(partial, TEAM, 0, 0, tiled=True)
    result = local_call(
        expand_kernel,
        array((ep, most, span)),
        summands.reshape(2, lines, peers, part, span),
        arrived,
    )
    returned = lax.all_to_all(result, EP, 0, 0, tiled=True)
    keep, send = local_call(
        combine_kernel,
        [array((tok, span), F32), array((tok, span))],
        mix,
        returned.reshape(layers, 2, most, span),
        place=place,
    )
    return (keep + lax.ppermute(send, ("g", "yy"), PAIR).astype(F32)).astype(BF)


def solution(mesh):
    torus = Mesh(mesh.devices.reshape(16, 2, 2, 2, 4), ("z", "c", "g", "yy", "x"))
    in_specs = (
        P(EP, None),
        P(None, EP),
        P(None, EP),
        P(EP, None, TP),
        P(EP, None, TP),
        P(EP, TP, None),
    )

    return jax.shard_map(
        per_device, mesh=torus, in_specs=in_specs, out_specs=P(EP, TP), check_vma=False
    )
```

```python
import jax
import jax.numpy as jnp
from jax import lax
from jax.experimental import pallas as pl
from jax.experimental.pallas import tpu as pltpu
from jax.sharding import Mesh
from jax.sharding import PartitionSpec as P

EP = ("z", "c")
TP = ("g", "yy", "x")
TEAM = ("c", "yy", "x")
BF = jnp.bfloat16
F32 = jnp.float32
EMPTY = 64.0
LIMIT = 32.0
TRADE = [(0, 0), (1, 1), (6, 6), (7, 7), (4, 3), (3, 4), (5, 2), (2, 5)]
PAIR = [(0, 3), (3, 0), (1, 2), (2, 1)]
ACROSS = [(k, k ^ 4) for k in range(8)] + [(k, k ^ 1) for k in range(8, 16)]
CORES = [(0, 1), (1, 0)]


def iota(shape, dim):
    return lax.broadcasted_iota(jnp.int32, shape, dim)


def dot(a, b):
    return jnp.dot(a, b, preferred_element_type=F32)


def one_hot(mask):
    return jnp.where(mask, 1.0, 0.0).astype(BF)


def whereabouts(place_ref):
    place = place_ref[0]
    return place // 8, place // 4, place % 4


def pack_kernel(gate_ref, up_ref, down_ref, out_ref, sems):
    _, width, span = gate_ref.shape
    copies = [(gate_ref.at[0], out_ref.at[:width]), (up_ref.at[0], out_ref.at[width : 2 * width])]
    for k in range(width // span):
        at = 2 * width + k * span
        copies.append((down_ref.at[0, :, k * span : (k + 1) * span], out_ref.at[at : at + span]))
    copies = [pltpu.make_async_copy(*c, sems.at[k]) for k, c in enumerate(copies)]
    for copy in copies:
        copy.start()
    for copy in copies:
        copy.wait()


def pick_kernel(place_ref, selected_ref, tokens_ref, rows_ref, tile_ref, out_ref, sems):
    g, y, x = whereabouts(place_ref)
    experts, most = selected_ref.shape
    _, tok, width = tile_ref.shape
    loads = []
    for c in range(2):
        block = 4 * ((jnp.minimum, jnp.maximum)[c](y, 3 - y)) + x
        at = pl.multiple_of(block * width, width)
        loads.append(
            pltpu.make_async_copy(tokens_ref.at[:, pl.ds(at, width)], tile_ref.at[c], sems.at[c])
        )
        loads[c].start()
    here = experts // 2
    slots = here * most
    sel = selected_ref[...].astype(F32).astype(BF)
    repeat = one_hot(2 * (iota((slots, experts), 0) // most) + g == iota((slots, experts), 1))
    own = iota((slots, most), 0) % most == iota((slots, most), 1)
    spread = jnp.where(own, dot(repeat, sel), 0.0).astype(BF)
    position = dot(spread, jnp.ones((most, tok), BF))
    named = one_hot(position == iota((slots, tok), 1).astype(F32))
    stores = []
    for c in range(2):
        loads[c].wait()
        rows = jnp.where(position < 0.0, EMPTY, dot(named, tile_ref[c])).astype(BF)
        out_ref[c] = rows.reshape(here, most, width)
        stores.append(pltpu.make_async_copy(out_ref.at[c], rows_ref.at[:, c], sems.at[2 + c]))
        stores[c].start()
    for store in stores:
        store.wait()


def mix_kernel(place_ref, selected_ref, affinity_ref, mix_ref):
    g, _, _ = whereabouts(place_ref)
    experts, most = selected_ref.shape
    _, tok, slots = mix_ref.shape
    sel = selected_ref[...].astype(F32).astype(BF)
    tile = one_hot(iota((most, slots), 0) == iota((most, slots), 1) % most)
    mine = iota((experts, slots), 0) == 2 * (iota((experts, slots), 1) // most) + g

    def as_row(values):
        return jnp.sum(jnp.where(mine, dot(values, tile), 0.0), axis=0, keepdims=True)

    aff = affinity_ref[...]
    high = aff.astype(BF)
    low = (aff - high.astype(F32)).astype(BF)
    hit = as_row(sel) == iota((tok, slots), 0).astype(F32)
    mix_ref[0] = jnp.where(hit, as_row(high), 0.0).astype(BF)
    mix_ref[1] = jnp.where(hit, as_row(low), 0.0).astype(BF)


def compact_kernel(slots_ref, rows_ref):
    blocks, most, width = slots_ref.shape
    cores, lines, peers, part, _ = rows_ref.shape
    slots = blocks * most
    count = 2 * cores * part
    data = slots_ref[...].reshape(slots, width)
    live = one_hot(data.astype(F32) < LIMIT)
    first = one_hot(iota((8, width), 1) == 0)
    live_row = lax.dot_general(first, live, (((1,), (1,)), ((), ())), preferred_element_type=F32)
    in_block = one_hot(iota((slots, blocks), 0) // most == iota((slots, blocks), 1))
    before = one_hot(iota((blocks, slots), 0) < iota((blocks, slots), 1) // most)
    counts = dot(live_row.astype(BF), in_block)
    rank = dot(counts.astype(BF), before) + (iota((8, slots), 1) % most).astype(F32)
    rank = jnp.where(live_row > 0.5, rank, -1.0)[0:1]
    take = one_hot(rank == iota((count, slots), 0).astype(F32))
    rows = dot(take, data).astype(BF)
    for c in range(cores):
        for k in range(lines):
            for x in range(peers):
                at = (2 * ((k + x) % 2) + c) * part
                rows_ref[c, k, x] = rows[at : at + part]


def seat(block, g):
    y = block // 4
    yy = (0, 1, 1, 0)[y]
    return (y // 2) * 8 + 4 * (yy + g - 2 * yy * g) + block % 4


def ffn_kernel(place_ref, x_ref, *refs):
    *weights, out_ref = refs
    g, _, _ = whereabouts(place_ref)
    peers, _, span = x_ref.shape
    width = peers * span
    x = jnp.concatenate([x_ref[seat(k, g)] for k in range(peers)], axis=1)
    gate = dot(x, jnp.concatenate([w[:width] for w in weights], axis=1))
    up = dot(x, jnp.concatenate([w[width : 2 * width] for w in weights], axis=1))
    hidden = (gate / (1.0 + jnp.exp(-gate)) * up).astype(BF)
    for k in range(0, peers, 2):
        at = 2 * width + k * span
        tiles = [
            jnp.concatenate([w[at + j * span : at + (j + 1) * span] for w in weights], axis=0)
            for j in range(2)
        ]
        partial = dot(hidden, jnp.concatenate(tiles, axis=1)).astype(BF)
        for j in range(2):
            out_ref[seat(k + j, g)] = partial[:, j * span : (j + 1) * span]


def expand_kernel(parts_ref, slots_ref, out_ref):
    cores, lines, peers, part, width = parts_ref.shape
    blocks, most, _ = slots_ref.shape
    slots = blocks * most
    quarters = []
    for half in range(2):
        for c in range(cores):
            total = jnp.zeros((part, width), F32)
            for k in range(lines):
                for x in range((half + k) % 2, peers, 2):
                    total = total + parts_ref[c, k, x].astype(F32)
            quarters.append(total.astype(BF))
    live = one_hot(slots_ref[...].reshape(slots, width).astype(F32) < LIMIT)
    in_block = one_hot(iota((blocks, slots), 0) == iota((blocks, slots), 1) // most)
    before = one_hot(iota((slots, blocks), 1) < iota((slots, blocks), 0) // most)
    counts = dot(in_block, live).astype(BF)
    rank = dot(before, counts) + (iota((slots, width), 0) % most).astype(F32)
    rank = jnp.where(live > 0.5, rank, -1.0)
    lanes = iota((slots, width), 1).astype(F32)
    put = [one_hot(rank - k == lanes) for k in range(0, 2 * cores * part, width)]
    rows = dot(jnp.concatenate(put, axis=1), jnp.concatenate(quarters, axis=0)).astype(BF)
    out_ref[...] = rows.reshape(blocks, most, width)


def combine_kernel(place_ref, mix_ref, rows_ref, keep_ref, send_ref):
    here, cores, most, width = rows_ref.shape
    both = [rows_ref[:, c].reshape(here * most, width) for c in range(cores)]
    both = jnp.concatenate(both, axis=1)
    total = dot(mix_ref[0], both) + dot(mix_ref[1], both)
    mine = whereabouts(place_ref)[0] == 0
    keep_ref[...] = jnp.where(mine, total[:, :width], total[:, width:])
    send_ref[...] = jnp.where(mine, total[:, width:], total[:, :width]).astype(BF)


def local_call(kernel, outs, *args, place=None, params=(), hbm=(), scratch=()):
    vmem = pl.BlockSpec(memory_space=pltpu.VMEM)
    specs = [pl.BlockSpec()] * len(params) + [vmem] * len(args)
    specs += [pl.BlockSpec(memory_space=pltpu.HBM)] * len(hbm)
    args = [pltpu.with_memory_space_constraint(a, pltpu.VMEM) for a in args]
    args = [*params, *args, *(pltpu.with_memory_space_constraint(a, pltpu.HBM) for a in hbm)]
    if place is not None:
        specs = [pl.BlockSpec(memory_space=pltpu.SMEM)] + specs
        args = [place] + args
    return pl.pallas_call(
        kernel,
        in_specs=specs,
        out_specs=jax.tree.map(lambda o: pl.BlockSpec(memory_space=o.memory_space), outs),
        out_shape=outs,
        scratch_shapes=scratch,
        compiler_params=pltpu.CompilerParams(vmem_limit_bytes=24 * 2**20),
    )(*args)


def array(shape, dtype=BF):
    return pltpu.VMEM(shape, dtype)


def per_device(tokens, selected, affinity, w_gate, w_up, w_down):
    ep = lax.axis_size(EP)
    layers = lax.axis_size("z")
    team = lax.axis_size(TEAM)
    tok, width = tokens.shape
    _, most = selected.shape
    span = width // team
    part = ep * most // 8
    lines = lax.axis_size("yy")
    peers = lax.axis_size("x")
    place = lax.axis_index(TP).astype(jnp.int32).reshape(1)
    packed = local_call(
        pack_kernel,
        array((3 * width, span)),
        hbm=(w_gate, w_up, w_down),
        scratch=[pltpu.SemaphoreType.DMA((2 + team,))],
    )
    mine = lax.ppermute(packed, ("c", "g", "yy"), TRADE)
    rows = local_call(
        pick_kernel,
        pltpu.HBM((layers, 2, most, span), BF),
        place=place,
        params=(selected,),
        hbm=(tokens,),
        scratch=[
            pltpu.VMEM((2, tok, span), BF),
            pltpu.VMEM((2, layers, most, span), BF),
            pltpu.SemaphoreType.DMA((4,)),
        ],
    )
    arrived = lax.all_to_all(rows.reshape(ep, most, span), EP, 0, 0, tiled=True)
    mix = local_call(
        mix_kernel,
        array((2, tok, layers * most)),
        place=place,
        params=(selected, affinity),
    )
    third = lax.ppermute(mine, ("c", "yy", "x"), ACROSS)
    other = lax.ppermute(mine, "c", CORES)
    copies = local_call(compact_kernel, array((2, lines, peers, part, span)), arrived)
    chosen = lax.all_to_all(copies.reshape(team, part, span), TEAM, 0, 0, tiled=True)
    fourth = lax.ppermute(third, "c", CORES)
    partial = local_call(
        ffn_kernel,
        array((team, part, span)),
        chosen,
        mine,
        other,
        third,
        fourth,
        place=place,
    )
    summands = lax.all_to_all(partial, TEAM, 0, 0, tiled=True)
    result = local_call(
        expand_kernel,
        array((ep, most, span)),
        summands.reshape(2, lines, peers, part, span),
        arrived,
    )
    returned = lax.all_to_all(result, EP, 0, 0, tiled=True)
    keep, send = local_call(
        combine_kernel,
        [array((tok, span), F32), array((tok, span))],
        mix,
        returned.reshape(layers, 2, most, span),
        place=place,
    )
    return (keep + lax.ppermute(send, ("g", "yy"), PAIR).astype(F32)).astype(BF)


def solution(mesh):
    torus = Mesh(mesh.devices.reshape(16, 2, 2, 2, 4), ("z", "c", "g", "yy", "x"))
    in_specs = (
        P(EP, None),
        P(None, EP),
        P(None, EP),
        P(EP, None, TP),
        P(EP, None, TP),
        P(EP, TP, None),
    )

    return jax.shard_map(
        per_device, mesh=torus, in_specs=in_specs, out_specs=P(EP, TP), check_vma=False
    )
```

```python
import jax
import jax.numpy as jnp
from jax import lax
from jax.experimental import pallas as pl
from jax.experimental.pallas import tpu as pltpu
from jax.sharding import Mesh
from jax.sharding import PartitionSpec as P

EP = ("z", "c")
TP = ("g", "yy", "x")
TEAM = ("c", "yy", "x")
BF = jnp.bfloat16
F32 = jnp.float32
EMPTY = 64.0
LIMIT = 32.0
TRADE = [(0, 0), (1, 1), (6, 6), (7, 7), (4, 3), (3, 4), (5, 2), (2, 5)]
PAIR = [(0, 3), (3, 0), (1, 2), (2, 1)]
CORES = [(0, 1), (1, 0)]


def iota(shape, dim):
    return lax.broadcasted_iota(jnp.int32, shape, dim)


def dot(a, b):
    return jnp.dot(a, b, preferred_element_type=F32)


def one_hot(mask):
    return jnp.where(mask, 1.0, 0.0).astype(BF)


def whereabouts(place_ref):
    place = place_ref[0]
    return place // 8, place // 4, place % 4


def pack_kernel(gate_ref, up_ref, down_ref, out_ref, sems):
    _, width, span = gate_ref.shape
    copies = [(gate_ref.at[0], out_ref.at[:width]), (up_ref.at[0], out_ref.at[width : 2 * width])]
    for k in range(width // span):
        at = 2 * width + k * span
        copies.append((down_ref.at[0, :, k * span : (k + 1) * span], out_ref.at[at : at + span]))
    copies = [pltpu.make_async_copy(*c, sems.at[k]) for k, c in enumerate(copies)]
    for copy in copies:
        copy.start()
    for copy in copies:
        copy.wait()


def pick_kernel(place_ref, selected_ref, tokens_ref, rows_ref, sel_ref, tile_ref, out_ref, sems):
    g, y, x = whereabouts(place_ref)
    experts, most = selected_ref.shape
    _, tok, width = tile_ref.shape
    first = pltpu.make_async_copy(selected_ref, sel_ref, sems.at[4])
    first.start()
    loads = []
    for c in range(2):
        block = 4 * ((jnp.minimum, jnp.maximum)[c](y, 3 - y)) + x
        at = pl.multiple_of(block * width, width)
        loads.append(
            pltpu.make_async_copy(tokens_ref.at[:, pl.ds(at, width)], tile_ref.at[c], sems.at[c])
        )
        loads[c].start()
    here = experts // 2
    slots = here * most
    first.wait()
    sel = sel_ref[...].astype(F32).astype(BF)
    repeat = one_hot(2 * (iota((slots, experts), 0) // most) + g == iota((slots, experts), 1))
    own = iota((slots, most), 0) % most == iota((slots, most), 1)
    spread = jnp.where(own, dot(repeat, sel), 0.0).astype(BF)
    position = dot(spread, jnp.ones((most, tok), BF))
    named = one_hot(position == iota((slots, tok), 1).astype(F32))
    stores = []
    for c in range(2):
        loads[c].wait()
        rows = jnp.where(position < 0.0, EMPTY, dot(named, tile_ref[c])).astype(BF)
        out_ref[c] = rows.reshape(here, most, width)
        stores.append(pltpu.make_async_copy(out_ref.at[c], rows_ref.at[:, c], sems.at[2 + c]))
        stores[c].start()
    for store in stores:
        store.wait()


def mix_kernel(place_ref, selected_ref, affinity_ref, mix_ref):
    g, _, _ = whereabouts(place_ref)
    experts, most = selected_ref.shape
    _, tok, slots = mix_ref.shape
    sel = selected_ref[...].astype(F32).astype(BF)
    tile = one_hot(iota((most, slots), 0) == iota((most, slots), 1) % most)
    mine = iota((experts, slots), 0) == 2 * (iota((experts, slots), 1) // most) + g

    def as_row(values):
        return jnp.sum(jnp.where(mine, dot(values, tile), 0.0), axis=0, keepdims=True)

    aff = affinity_ref[...]
    high = aff.astype(BF)
    low = (aff - high.astype(F32)).astype(BF)
    hit = as_row(sel) == iota((tok, slots), 0).astype(F32)
    mix_ref[0] = jnp.where(hit, as_row(high), 0.0).astype(BF)
    mix_ref[1] = jnp.where(hit, as_row(low), 0.0).astype(BF)


def compact_kernel(slots_ref, rows_ref):
    blocks, most, width = slots_ref.shape
    cores, lines, peers, part, _ = rows_ref.shape
    slots = blocks * most
    count = cores * part
    data = slots_ref[...].reshape(slots, width)
    live = one_hot(data.astype(F32) < LIMIT)
    first = one_hot(iota((8, width), 1) == 0)
    live_row = lax.dot_general(first, live, (((1,), (1,)), ((), ())), preferred_element_type=F32)
    in_block = one_hot(iota((slots, blocks), 0) // most == iota((slots, blocks), 1))
    before = one_hot(iota((blocks, slots), 0) < iota((blocks, slots), 1) // most)
    counts = dot(live_row.astype(BF), in_block)
    rank = dot(counts.astype(BF), before) + (iota((8, slots), 1) % most).astype(F32)
    rank = jnp.where(live_row > 0.5, rank, -1.0)[0:1]
    take = one_hot(rank == iota((count, slots), 0).astype(F32))
    rows = dot(take, data).astype(BF)
    for c in range(cores):
        for k in range(lines):
            for x in range(peers):
                rows_ref[c, k, x] = rows[c * part : (c + 1) * part]


def seat(block, g):
    y = block // 4
    yy = (0, 1, 1, 0)[y]
    return (y // 2) * 8 + 4 * (yy + g - 2 * yy * g) + block % 4


def ffn_kernel(place_ref, x_ref, *refs):
    *weights, out_ref = refs
    g, _, _ = whereabouts(place_ref)
    peers, _, span = x_ref.shape
    width = peers * span
    x = jnp.concatenate([x_ref[seat(k, g)] for k in range(peers)], axis=1)
    gate = dot(x, jnp.concatenate([w[:width] for w in weights], axis=1))
    up = dot(x, jnp.concatenate([w[width : 2 * width] for w in weights], axis=1))
    hidden = (gate / (1.0 + jnp.exp(-gate)) * up).astype(BF)
    for k in range(0, peers, 2):
        at = 2 * width + k * span
        tiles = [
            jnp.concatenate([w[at + j * span : at + (j + 1) * span] for w in weights], axis=0)
            for j in range(2)
        ]
        partial = dot(hidden, jnp.concatenate(tiles, axis=1)).astype(BF)
        for j in range(2):
            out_ref[seat(k + j, g)] = partial[:, j * span : (j + 1) * span]


def expand_kernel(parts_ref, slots_ref, out_ref):
    cores, lines, peers, part, width = parts_ref.shape
    blocks, most, _ = slots_ref.shape
    slots = blocks * most
    halves = []
    for c in range(cores):
        total = jnp.zeros((part, width), F32)
        for k in range(lines):
            for x in range(peers):
                total = total + parts_ref[c, k, x].astype(F32)
        halves.append(total.astype(BF))
    live = one_hot(slots_ref[...].reshape(slots, width).astype(F32) < LIMIT)
    in_block = one_hot(iota((blocks, slots), 0) == iota((blocks, slots), 1) // most)
    before = one_hot(iota((slots, blocks), 1) < iota((slots, blocks), 0) // most)
    counts = dot(in_block, live).astype(BF)
    rank = dot(before, counts) + (iota((slots, width), 0) % most).astype(F32)
    rank = jnp.where(live > 0.5, rank, -1.0)
    lanes = iota((slots, width), 1).astype(F32)
    put = [one_hot(rank - k == lanes) for k in range(0, cores * part, width)]
    rows = dot(jnp.concatenate(put, axis=1), jnp.concatenate(halves, axis=0)).astype(BF)
    out_ref[...] = rows.reshape(blocks, most, width)


def combine_kernel(place_ref, mix_ref, rows_ref, keep_ref, send_ref):
    here, cores, most, width = rows_ref.shape
    both = [rows_ref[:, c].reshape(here * most, width) for c in range(cores)]
    both = jnp.concatenate(both, axis=1)
    total = dot(mix_ref[0], both) + dot(mix_ref[1], both)
    mine = whereabouts(place_ref)[0] == 0
    keep_ref[...] = jnp.where(mine, total[:, :width], total[:, width:])
    send_ref[...] = jnp.where(mine, total[:, width:], total[:, :width]).astype(BF)


def local_call(kernel, outs, *args, place=None, params=(), hbm=(), scratch=()):
    vmem = pl.BlockSpec(memory_space=pltpu.VMEM)
    specs = [pl.BlockSpec()] * len(params) + [vmem] * len(args)
    specs += [pl.BlockSpec(memory_space=pltpu.HBM)] * len(hbm)
    args = [pltpu.with_memory_space_constraint(a, pltpu.VMEM) for a in args]
    args = [*params, *args, *(pltpu.with_memory_space_constraint(a, pltpu.HBM) for a in hbm)]
    if place is not None:
        specs = [pl.BlockSpec(memory_space=pltpu.SMEM)] + specs
        args = [place] + args
    return pl.pallas_call(
        kernel,
        in_specs=specs,
        out_specs=jax.tree.map(lambda o: pl.BlockSpec(memory_space=o.memory_space), outs),
        out_shape=outs,
        scratch_shapes=scratch,
        compiler_params=pltpu.CompilerParams(vmem_limit_bytes=24 * 2**20),
    )(*args)


def array(shape, dtype=BF):
    return pltpu.VMEM(shape, dtype)


def per_device(tokens, selected, affinity, w_gate, w_up, w_down):
    ep = lax.axis_size(EP)
    layers = lax.axis_size("z")
    team = lax.axis_size(TEAM)
    tok, width = tokens.shape
    experts, most = selected.shape
    span = width // team
    part = ep * most // 4
    lines = lax.axis_size("yy")
    peers = lax.axis_size("x")
    place = lax.axis_index(TP).astype(jnp.int32).reshape(1)
    packed = local_call(
        pack_kernel,
        array((3 * width, span)),
        hbm=(w_gate, w_up, w_down),
        scratch=[pltpu.SemaphoreType.DMA((2 + team,))],
    )
    mine = lax.ppermute(packed, ("c", "g", "yy"), TRADE)
    rows = local_call(
        pick_kernel,
        pltpu.HBM((layers, 2, most, span), BF),
        place=place,
        hbm=(selected, tokens),
        scratch=[
            pltpu.VMEM((experts, most), jnp.int32),
            pltpu.VMEM((2, tok, span), BF),
            pltpu.VMEM((2, layers, most, span), BF),
            pltpu.SemaphoreType.DMA((5,)),
        ],
    )
    arrived = lax.all_to_all(rows.reshape(ep, most, span), EP, 0, 0, tiled=True)
    mix = local_call(
        mix_kernel,
        array((2, tok, layers * most)),
        place=place,
        params=(selected, affinity),
    )
    other = lax.ppermute(mine, "c", CORES)
    copies = local_call(compact_kernel, array((2, lines, peers, part, span)), arrived)
    chosen = lax.all_to_all(copies.reshape(team, part, span), TEAM, 0, 0, tiled=True)
    partial = local_call(ffn_kernel, array((team, part, span)), chosen, mine, other, place=place)
    summands = lax.all_to_all(partial, TEAM, 0, 0, tiled=True)
    result = local_call(
        expand_kernel,
        array((ep, most, span)),
        summands.reshape(2, lines, peers, part, span),
        arrived,
    )
    returned = lax.all_to_all(result, EP, 0, 0, tiled=True)
    keep, send = local_call(
        combine_kernel,
        [array((tok, span), F32), array((tok, span))],
        mix,
        returned.reshape(layers, 2, most, span),
        place=place,
    )
    return (keep + lax.ppermute(send, ("g", "yy"), PAIR).astype(F32)).astype(BF)


def solution(mesh):
    torus = Mesh(mesh.devices.reshape(16, 2, 2, 2, 4), ("z", "c", "g", "yy", "x"))
    in_specs = (
        P(EP, None),
        P(None, EP),
        P(None, EP),
        P(EP, None, TP),
        P(EP, None, TP),
        P(EP, TP, None),
    )

    return jax.shard_map(
        per_device, mesh=torus, in_specs=in_specs, out_specs=P(EP, TP), check_vma=False
    )
```

```python
import jax
import jax.numpy as jnp
from jax import lax
from jax.experimental import pallas as pl
from jax.experimental.pallas import tpu as pltpu
from jax.sharding import Mesh
from jax.sharding import PartitionSpec as P

EP = ("z", "c")
TP = ("g", "yy", "x")
TEAM = ("c", "yy", "x")
BF = jnp.bfloat16
F32 = jnp.float32
EMPTY = 64.0
LIMIT = 32.0
TRADE = [(0, 0), (1, 1), (6, 6), (7, 7), (4, 3), (3, 4), (5, 2), (2, 5)]
PAIR = [(0, 3), (3, 0), (1, 2), (2, 1)]
CORES = [(0, 1), (1, 0)]


def iota(shape, dim):
    return lax.broadcasted_iota(jnp.int32, shape, dim)


def dot(a, b):
    return jnp.dot(a, b, preferred_element_type=F32)


def one_hot(mask):
    return jnp.where(mask, 1.0, 0.0).astype(BF)


def whereabouts(place_ref):
    place = place_ref[0]
    return place // 8, place // 4, place % 4


def pack_kernel(gate_ref, up_ref, down_ref, out_ref, sems):
    _, width, span = gate_ref.shape
    copies = [(gate_ref.at[0], out_ref.at[:width]), (up_ref.at[0], out_ref.at[width : 2 * width])]
    for k in range(width // span):
        at = 2 * width + k * span
        copies.append((down_ref.at[0, :, k * span : (k + 1) * span], out_ref.at[at : at + span]))
    copies = [pltpu.make_async_copy(*c, sems.at[k]) for k, c in enumerate(copies)]
    for copy in copies:
        copy.start()
    for copy in copies:
        copy.wait()


def pick_kernel(place_ref, selected_ref, tokens_ref, rows_ref, sel_ref, tile_ref, out_ref, sems):
    g, y, x = whereabouts(place_ref)
    experts, most = selected_ref.shape
    _, tok, width = tile_ref.shape
    first = pltpu.make_async_copy(selected_ref, sel_ref, sems.at[4])
    first.start()
    loads = []
    for c in range(2):
        block = 4 * ((jnp.minimum, jnp.maximum)[c](y, 3 - y)) + x
        at = pl.multiple_of(block * width, width)
        loads.append(
            pltpu.make_async_copy(tokens_ref.at[:, pl.ds(at, width)], tile_ref.at[c], sems.at[c])
        )
        loads[c].start()
    here = experts // 2
    slots = here * most
    first.wait()
    sel = sel_ref[...].astype(F32).astype(BF)
    repeat = one_hot(2 * (iota((slots, experts), 0) // most) + g == iota((slots, experts), 1))
    own = iota((slots, most), 0) % most == iota((slots, most), 1)
    spread = jnp.where(own, dot(repeat, sel), 0.0).astype(BF)
    position = dot(spread, jnp.ones((most, tok), BF))
    named = one_hot(position == iota((slots, tok), 1).astype(F32))
    stores = []
    for c in range(2):
        loads[c].wait()
        rows = jnp.where(position < 0.0, EMPTY, dot(named, tile_ref[c])).astype(BF)
        out_ref[c] = rows.reshape(here, most, width)
        stores.append(pltpu.make_async_copy(out_ref.at[c], rows_ref.at[:, c], sems.at[2 + c]))
        stores[c].start()
    for store in stores:
        store.wait()


def mix_kernel(place_ref, selected_ref, affinity_ref, mix_ref):
    g, _, _ = whereabouts(place_ref)
    experts, most = selected_ref.shape
    _, tok, slots = mix_ref.shape
    sel = selected_ref[...].astype(F32).astype(BF)
    tile = one_hot(iota((most, slots), 0) == iota((most, slots), 1) % most)
    mine = iota((experts, slots), 0) == 2 * (iota((experts, slots), 1) // most) + g

    def as_row(values):
        return jnp.sum(jnp.where(mine, dot(values, tile), 0.0), axis=0, keepdims=True)

    aff = affinity_ref[...]
    high = aff.astype(BF)
    low = (aff - high.astype(F32)).astype(BF)
    hit = as_row(sel) == iota((tok, slots), 0).astype(F32)
    mix_ref[0] = jnp.where(hit, as_row(high), 0.0).astype(BF)
    mix_ref[1] = jnp.where(hit, as_row(low), 0.0).astype(BF)


def compact_kernel(slots_ref, rows_ref, half_ref, sems):
    blocks, most, width = slots_ref.shape
    cores, lines, peers, part, _ = rows_ref.shape
    slots = blocks * most
    count = cores * part
    data = slots_ref[...].reshape(slots, width)
    live = one_hot(data.astype(F32) < LIMIT)
    first = one_hot(iota((8, width), 1) == 0)
    live_row = lax.dot_general(first, live, (((1,), (1,)), ((), ())), preferred_element_type=F32)
    in_block = one_hot(iota((slots, blocks), 0) // most == iota((slots, blocks), 1))
    before = one_hot(iota((blocks, slots), 0) < iota((blocks, slots), 1) // most)
    counts = dot(live_row.astype(BF), in_block)
    rank = dot(counts.astype(BF), before) + (iota((8, slots), 1) % most).astype(F32)
    rank = jnp.where(live_row > 0.5, rank, -1.0)[0:1]
    take = one_hot(rank == iota((count, slots), 0).astype(F32))
    copies = []
    for c in range(cores):
        half_ref[c] = dot(take[c * part : (c + 1) * part], data).astype(BF)
        for k in range(lines):
            for x in range(peers):
                sem = sems.at[len(copies)]
                copies.append(pltpu.make_async_copy(half_ref.at[c], rows_ref.at[c, k, x], sem))
                copies[-1].start()
    for copy in copies:
        copy.wait()


def seat(block, g):
    y = block // 4
    yy = (0, 1, 1, 0)[y]
    return (y // 2) * 8 + 4 * (yy + g - 2 * yy * g) + block % 4


def ffn_kernel(place_ref, x_ref, mine_ref, other_ref, out_ref, local_ref, sems):
    g, _, _ = whereabouts(place_ref)
    peers, _, span = x_ref.shape
    width = peers * span
    loads = []
    for k in range(3):
        part = pl.ds(k * width, width)
        loads.append(pltpu.make_async_copy(other_ref.at[part], local_ref.at[part], sems.at[k]))
        loads[k].start()
    x = jnp.concatenate([x_ref[seat(k, g)] for k in range(peers)], axis=1)
    hidden = []
    for w in (mine_ref, local_ref):
        if w is local_ref:
            loads[0].wait()
            loads[1].wait()
        both = dot(x, jnp.concatenate([w[:width], w[width : 2 * width]], axis=1))
        gate = both[:, :span]
        hidden.append((gate / (1.0 + jnp.exp(-gate)) * both[:, span:]).astype(BF))
    hidden = jnp.concatenate(hidden, axis=1)
    loads[2].wait()
    for k in range(0, peers, 2):
        at = 2 * width + k * span
        tiles = [
            jnp.concatenate(
                [w[at + j * span : at + (j + 1) * span] for w in (mine_ref, local_ref)], axis=0
            )
            for j in range(2)
        ]
        partial = dot(hidden, jnp.concatenate(tiles, axis=1)).astype(BF)
        for j in range(2):
            out_ref[seat(k + j, g)] = partial[:, j * span : (j + 1) * span]


def expand_kernel(parts_ref, slots_ref, out_ref):
    cores, lines, peers, part, width = parts_ref.shape
    blocks, most, _ = slots_ref.shape
    slots = blocks * most
    halves = []
    for c in range(cores):
        total = jnp.zeros((part, width), F32)
        for k in range(lines):
            for x in range(peers):
                total = total + parts_ref[c, k, x].astype(F32)
        halves.append(total.astype(BF))
    live = one_hot(slots_ref[...].reshape(slots, width).astype(F32) < LIMIT)
    in_block = one_hot(iota((blocks, slots), 0) == iota((blocks, slots), 1) // most)
    before = one_hot(iota((slots, blocks), 1) < iota((slots, blocks), 0) // most)
    counts = dot(in_block, live).astype(BF)
    rank = dot(before, counts) + (iota((slots, width), 0) % most).astype(F32)
    rank = jnp.where(live > 0.5, rank, -1.0)
    lanes = iota((slots, width), 1).astype(F32)
    put = [one_hot(rank - k == lanes) for k in range(0, cores * part, width)]
    rows = dot(jnp.concatenate(put, axis=1), jnp.concatenate(halves, axis=0)).astype(BF)
    out_ref[...] = rows.reshape(blocks, most, width)


def combine_kernel(place_ref, mix_ref, rows_ref, keep_ref, send_ref):
    here, cores, most, width = rows_ref.shape
    both = [rows_ref[:, c].reshape(here * most, width) for c in range(cores)]
    both = jnp.concatenate(both, axis=1)
    total = dot(mix_ref[0], both) + dot(mix_ref[1], both)
    mine = whereabouts(place_ref)[0] == 0
    keep_ref[...] = jnp.where(mine, total[:, :width], total[:, width:])
    send_ref[...] = jnp.where(mine, total[:, width:], total[:, :width]).astype(BF)


def local_call(kernel, outs, *args, place=None, params=(), hbm=(), scratch=()):
    vmem = pl.BlockSpec(memory_space=pltpu.VMEM)
    specs = [pl.BlockSpec()] * len(params) + [vmem] * len(args)
    specs += [pl.BlockSpec(memory_space=pltpu.HBM)] * len(hbm)
    args = [pltpu.with_memory_space_constraint(a, pltpu.VMEM) for a in args]
    args = [*params, *args, *(pltpu.with_memory_space_constraint(a, pltpu.HBM) for a in hbm)]
    if place is not None:
        specs = [pl.BlockSpec(memory_space=pltpu.SMEM)] + specs
        args = [place] + args
    return pl.pallas_call(
        kernel,
        in_specs=specs,
        out_specs=jax.tree.map(lambda o: pl.BlockSpec(memory_space=o.memory_space), outs),
        out_shape=outs,
        scratch_shapes=scratch,
        compiler_params=pltpu.CompilerParams(vmem_limit_bytes=24 * 2**20),
    )(*args)


def array(shape, dtype=BF):
    return pltpu.VMEM(shape, dtype)


def per_device(tokens, selected, affinity, w_gate, w_up, w_down):
    ep = lax.axis_size(EP)
    layers = lax.axis_size("z")
    team = lax.axis_size(TEAM)
    tok, width = tokens.shape
    experts, most = selected.shape
    span = width // team
    part = ep * most // 4
    lines = lax.axis_size("yy")
    peers = lax.axis_size("x")
    place = lax.axis_index(TP).astype(jnp.int32).reshape(1)
    packed = local_call(
        pack_kernel,
        pltpu.HBM((3 * width, span), BF),
        hbm=(w_gate, w_up, w_down),
        scratch=[pltpu.SemaphoreType.DMA((2 + team,))],
    )
    mine = lax.ppermute(packed, ("c", "g", "yy"), TRADE)
    rows = local_call(
        pick_kernel,
        pltpu.HBM((layers, 2, most, span), BF),
        place=place,
        hbm=(selected, tokens),
        scratch=[
            pltpu.VMEM((experts, most), jnp.int32),
            pltpu.VMEM((2, tok, span), BF),
            pltpu.VMEM((2, layers, most, span), BF),
            pltpu.SemaphoreType.DMA((5,)),
        ],
    )
    arrived = lax.all_to_all(rows.reshape(ep, most, span), EP, 0, 0, tiled=True)
    mix = local_call(
        mix_kernel,
        array((2, tok, layers * most)),
        place=place,
        params=(selected, affinity),
    )
    other = lax.ppermute(mine, "c", CORES)
    copies = local_call(
        compact_kernel,
        pltpu.HBM((2, lines, peers, part, span), BF),
        arrived,
        scratch=[pltpu.VMEM((2, part, span), BF), pltpu.SemaphoreType.DMA((team,))],
    )
    chosen = lax.all_to_all(copies.reshape(team, part, span), TEAM, 0, 0, tiled=True)
    partial = local_call(
        ffn_kernel,
        array((team, part, span)),
        chosen,
        mine,
        place=place,
        hbm=(other,),
        scratch=[pltpu.VMEM((3 * width, span), BF), pltpu.SemaphoreType.DMA((3,))],
    )
    summands = lax.all_to_all(partial, TEAM, 0, 0, tiled=True)
    result = local_call(
        expand_kernel,
        array((ep, most, span)),
        summands.reshape(2, lines, peers, part, span),
        arrived,
    )
    returned = lax.all_to_all(result, EP, 0, 0, tiled=True)
    keep, send = local_call(
        combine_kernel,
        [array((tok, span), F32), array((tok, span))],
        mix,
        returned.reshape(layers, 2, most, span),
        place=place,
    )
    return (keep + lax.ppermute(send, ("g", "yy"), PAIR).astype(F32)).astype(BF)


def solution(mesh):
    torus = Mesh(mesh.devices.reshape(16, 2, 2, 2, 4), ("z", "c", "g", "yy", "x"))
    in_specs = (
        P(EP, None),
        P(None, EP),
        P(None, EP),
        P(EP, None, TP),
        P(EP, None, TP),
        P(EP, TP, None),
    )

    return jax.shard_map(
        per_device, mesh=torus, in_specs=in_specs, out_specs=P(EP, TP), check_vma=False
    )
```

```python
import jax
import jax.numpy as jnp
from jax import lax
from jax.experimental import pallas as pl
from jax.experimental.pallas import tpu as pltpu
from jax.sharding import Mesh
from jax.sharding import PartitionSpec as P

EP = ("z", "c")
TP = ("g", "yy", "x")
TEAM = ("c", "yy", "x")
BF = jnp.bfloat16
F32 = jnp.float32
EMPTY = 64.0
LIMIT = 32.0
TRADE = [(0, 0), (1, 1), (6, 6), (7, 7), (4, 3), (3, 4), (5, 2), (2, 5)]
PAIR = [(0, 3), (3, 0), (1, 2), (2, 1)]
CORES = [(0, 1), (1, 0)]


def iota(shape, dim):
    return lax.broadcasted_iota(jnp.int32, shape, dim)


def dot(a, b):
    return jnp.dot(a, b, preferred_element_type=F32)


def one_hot(mask):
    return jnp.where(mask, 1.0, 0.0).astype(BF)


def whereabouts(place_ref):
    place = place_ref[0]
    return place // 8, place // 4, place % 4


def pick_kernel(
    place_ref,
    selected_ref,
    tokens_ref,
    gate_ref,
    up_ref,
    down_ref,
    rows_ref,
    packed_ref,
    sel_ref,
    tile_ref,
    out_ref,
    sems,
    pack_sems,
):
    g, y, x = whereabouts(place_ref)
    experts, most = selected_ref.shape
    _, tok, width = tile_ref.shape
    first = pltpu.make_async_copy(selected_ref, sel_ref, sems.at[4])
    first.start()
    loads = []
    for c in range(2):
        block = 4 * ((jnp.minimum, jnp.maximum)[c](y, 3 - y)) + x
        at = pl.multiple_of(block * width, width)
        loads.append(
            pltpu.make_async_copy(tokens_ref.at[:, pl.ds(at, width)], tile_ref.at[c], sems.at[c])
        )
        loads[c].start()
    _, full, span = gate_ref.shape
    pieces = [(gate_ref.at[0], packed_ref.at[:full])]
    pieces.append((up_ref.at[0], packed_ref.at[full : 2 * full]))
    for k in range(full // span):
        at = 2 * full + k * span
        piece = down_ref.at[0, :, k * span : (k + 1) * span]
        pieces.append((piece, packed_ref.at[at : at + span]))
    pieces = [pltpu.make_async_copy(*p, pack_sems.at[k]) for k, p in enumerate(pieces)]
    for piece in pieces:
        piece.start()
    here = experts // 2
    slots = here * most
    first.wait()
    sel = sel_ref[...].astype(F32).astype(BF)
    repeat = one_hot(2 * (iota((slots, experts), 0) // most) + g == iota((slots, experts), 1))
    own = iota((slots, most), 0) % most == iota((slots, most), 1)
    spread = jnp.where(own, dot(repeat, sel), 0.0).astype(BF)
    position = dot(spread, jnp.ones((most, tok), BF))
    named = one_hot(position == iota((slots, tok), 1).astype(F32))
    stores = []
    for c in range(2):
        loads[c].wait()
        rows = jnp.where(position < 0.0, EMPTY, dot(named, tile_ref[c])).astype(BF)
        out_ref[c] = rows.reshape(here, most, width)
        stores.append(pltpu.make_async_copy(out_ref.at[c], rows_ref.at[:, c], sems.at[2 + c]))
        stores[c].start()
    for copy in stores + pieces:
        copy.wait()


def mix_kernel(place_ref, selected_ref, affinity_ref, mix_ref):
    g, _, _ = whereabouts(place_ref)
    experts, most = selected_ref.shape
    _, tok, slots = mix_ref.shape
    sel = selected_ref[...].astype(F32).astype(BF)
    tile = one_hot(iota((most, slots), 0) == iota((most, slots), 1) % most)
    mine = iota((experts, slots), 0) == 2 * (iota((experts, slots), 1) // most) + g

    def as_row(values):
        return jnp.sum(jnp.where(mine, dot(values, tile), 0.0), axis=0, keepdims=True)

    aff = affinity_ref[...]
    high = aff.astype(BF)
    low = (aff - high.astype(F32)).astype(BF)
    hit = as_row(sel) == iota((tok, slots), 0).astype(F32)
    mix_ref[0] = jnp.where(hit, as_row(high), 0.0).astype(BF)
    mix_ref[1] = jnp.where(hit, as_row(low), 0.0).astype(BF)


def compact_kernel(slots_ref, rows_ref):
    blocks, most, width = slots_ref.shape
    cores, lines, peers, part, _ = rows_ref.shape
    slots = blocks * most
    count = cores * part
    data = slots_ref[...].reshape(slots, width)
    live = one_hot(data.astype(F32) < LIMIT)
    first = one_hot(iota((8, width), 1) == 0)
    live_row = lax.dot_general(first, live, (((1,), (1,)), ((), ())), preferred_element_type=F32)
    in_block = one_hot(iota((slots, blocks), 0) // most == iota((slots, blocks), 1))
    before = one_hot(iota((blocks, slots), 0) < iota((blocks, slots), 1) // most)
    counts = dot(live_row.astype(BF), in_block)
    rank = dot(counts.astype(BF), before) + (iota((8, slots), 1) % most).astype(F32)
    rank = jnp.where(live_row > 0.5, rank, -1.0)[0:1]
    take = one_hot(rank == iota((count, slots), 0).astype(F32))
    rows = dot(take, data).astype(BF)
    for c in range(cores):
        for k in range(lines):
            for x in range(peers):
                rows_ref[c, k, x] = rows[c * part : (c + 1) * part]


def seat(block, g):
    y = block // 4
    yy = (0, 1, 1, 0)[y]
    return (y // 2) * 8 + 4 * (yy + g - 2 * yy * g) + block % 4


def ffn_kernel(place_ref, x_ref, *refs):
    *weights, out_ref = refs
    g, _, _ = whereabouts(place_ref)
    peers, _, span = x_ref.shape
    width = peers * span
    x = jnp.concatenate([x_ref[seat(k, g)] for k in range(peers)], axis=1)
    gate = dot(x, jnp.concatenate([w[:width] for w in weights], axis=1))
    up = dot(x, jnp.concatenate([w[width : 2 * width] for w in weights], axis=1))
    hidden = (gate / (1.0 + jnp.exp(-gate)) * up).astype(BF)
    for k in range(0, peers, 2):
        at = 2 * width + k * span
        tiles = [
            jnp.concatenate([w[at + j * span : at + (j + 1) * span] for w in weights], axis=0)
            for j in range(2)
        ]
        partial = dot(hidden, jnp.concatenate(tiles, axis=1)).astype(BF)
        for j in range(2):
            out_ref[seat(k + j, g)] = partial[:, j * span : (j + 1) * span]


def expand_kernel(parts_ref, slots_ref, out_ref):
    cores, lines, peers, part, width = parts_ref.shape
    blocks, most, _ = slots_ref.shape
    slots = blocks * most
    halves = []
    for c in range(cores):
        total = jnp.zeros((part, width), F32)
        for k in range(lines):
            for x in range(peers):
                total = total + parts_ref[c, k, x].astype(F32)
        halves.append(total.astype(BF))
    live = one_hot(slots_ref[...].reshape(slots, width).astype(F32) < LIMIT)
    in_block = one_hot(iota((blocks, slots), 0) == iota((blocks, slots), 1) // most)
    before = one_hot(iota((slots, blocks), 1) < iota((slots, blocks), 0) // most)
    counts = dot(in_block, live).astype(BF)
    rank = dot(before, counts) + (iota((slots, width), 0) % most).astype(F32)
    rank = jnp.where(live > 0.5, rank, -1.0)
    lanes = iota((slots, width), 1).astype(F32)
    put = [one_hot(rank - k == lanes) for k in range(0, cores * part, width)]
    rows = dot(jnp.concatenate(put, axis=1), jnp.concatenate(halves, axis=0)).astype(BF)
    out_ref[...] = rows.reshape(blocks, most, width)


def combine_kernel(place_ref, mix_ref, rows_ref, keep_ref, send_ref):
    here, cores, most, width = rows_ref.shape
    both = [rows_ref[:, c].reshape(here * most, width) for c in range(cores)]
    both = jnp.concatenate(both, axis=1)
    total = dot(mix_ref[0], both) + dot(mix_ref[1], both)
    mine = whereabouts(place_ref)[0] == 0
    keep_ref[...] = jnp.where(mine, total[:, :width], total[:, width:])
    send_ref[...] = jnp.where(mine, total[:, width:], total[:, :width]).astype(BF)


def local_call(kernel, outs, *args, place=None, params=(), hbm=(), scratch=()):
    vmem = pl.BlockSpec(memory_space=pltpu.VMEM)
    specs = [pl.BlockSpec()] * len(params) + [vmem] * len(args)
    specs += [pl.BlockSpec(memory_space=pltpu.HBM)] * len(hbm)
    args = [pltpu.with_memory_space_constraint(a, pltpu.VMEM) for a in args]
    args = [*params, *args, *(pltpu.with_memory_space_constraint(a, pltpu.HBM) for a in hbm)]
    if place is not None:
        specs = [pl.BlockSpec(memory_space=pltpu.SMEM)] + specs
        args = [place] + args
    return pl.pallas_call(
        kernel,
        in_specs=specs,
        out_specs=jax.tree.map(lambda o: pl.BlockSpec(memory_space=o.memory_space), outs),
        out_shape=outs,
        scratch_shapes=scratch,
        compiler_params=pltpu.CompilerParams(vmem_limit_bytes=24 * 2**20),
    )(*args)


def array(shape, dtype=BF):
    return pltpu.VMEM(shape, dtype)


def per_device(tokens, selected, affinity, w_gate, w_up, w_down):
    ep = lax.axis_size(EP)
    layers = lax.axis_size("z")
    team = lax.axis_size(TEAM)
    tok, width = tokens.shape
    experts, most = selected.shape
    span = width // team
    part = ep * most // 4
    lines = lax.axis_size("yy")
    peers = lax.axis_size("x")
    place = lax.axis_index(TP).astype(jnp.int32).reshape(1)
    rows, packed = local_call(
        pick_kernel,
        [pltpu.HBM((layers, 2, most, span), BF), array((3 * width, span))],
        place=place,
        hbm=(selected, tokens, w_gate, w_up, w_down),
        scratch=[
            pltpu.VMEM((experts, most), jnp.int32),
            pltpu.VMEM((2, tok, span), BF),
            pltpu.VMEM((2, layers, most, span), BF),
            pltpu.SemaphoreType.DMA((5,)),
            pltpu.SemaphoreType.DMA((2 + team,)),
        ],
    )
    mine = lax.ppermute(packed, ("c", "g", "yy"), TRADE)
    arrived = lax.all_to_all(rows.reshape(ep, most, span), EP, 0, 0, tiled=True)
    mix = local_call(
        mix_kernel,
        array((2, tok, layers * most)),
        place=place,
        params=(selected, affinity),
    )
    other = lax.ppermute(mine, "c", CORES)
    copies = local_call(compact_kernel, array((2, lines, peers, part, span)), arrived)
    chosen = lax.all_to_all(copies.reshape(team, part, span), TEAM, 0, 0, tiled=True)
    partial = local_call(ffn_kernel, array((team, part, span)), chosen, mine, other, place=place)
    summands = lax.all_to_all(partial, TEAM, 0, 0, tiled=True)
    result = local_call(
        expand_kernel,
        array((ep, most, span)),
        summands.reshape(2, lines, peers, part, span),
        arrived,
    )
    returned = lax.all_to_all(result, EP, 0, 0, tiled=True)
    keep, send = local_call(
        combine_kernel,
        [array((tok, span), F32), array((tok, span))],
        mix,
        returned.reshape(layers, 2, most, span),
        place=place,
    )
    return (keep + lax.ppermute(send, ("g", "yy"), PAIR).astype(F32)).astype(BF)


def solution(mesh):
    torus = Mesh(mesh.devices.reshape(16, 2, 2, 2, 4), ("z", "c", "g", "yy", "x"))
    in_specs = (
        P(EP, None),
        P(None, EP),
        P(None, EP),
        P(EP, None, TP),
        P(EP, None, TP),
        P(EP, TP, None),
    )

    return jax.shard_map(
        per_device, mesh=torus, in_specs=in_specs, out_specs=P(EP, TP), check_vma=False
    )
```

```python
import jax
import jax.numpy as jnp
from jax import lax
from jax.experimental import pallas as pl
from jax.experimental.pallas import tpu as pltpu
from jax.sharding import Mesh
from jax.sharding import PartitionSpec as P

EP = ("z", "c")
TP = ("g", "yy", "x")
TEAM = ("c", "yy", "x")
BF = jnp.bfloat16
F32 = jnp.float32
EMPTY = 64.0
LIMIT = 32.0
TRADE = [(0, 0), (1, 1), (6, 6), (7, 7), (4, 3), (3, 4), (5, 2), (2, 5)]
CORES = [(0, 1), (1, 0)]


def iota(shape, dim):
    return lax.broadcasted_iota(jnp.int32, shape, dim)


def dot(a, b):
    return jnp.dot(a, b, preferred_element_type=F32)


def one_hot(mask):
    return jnp.where(mask, 1.0, 0.0).astype(BF)


def whereabouts(place_ref):
    place = place_ref[0]
    return place // 8, place // 4, place % 4


def pack_kernel(gate_ref, up_ref, down_ref, out_ref, sems):
    _, width, span = gate_ref.shape
    copies = [(gate_ref.at[0], out_ref.at[:width]), (up_ref.at[0], out_ref.at[width : 2 * width])]
    for k in range(width // span):
        at = 2 * width + k * span
        copies.append((down_ref.at[0, :, k * span : (k + 1) * span], out_ref.at[at : at + span]))
    copies = [pltpu.make_async_copy(*c, sems.at[k]) for k, c in enumerate(copies)]
    for copy in copies:
        copy.start()
    for copy in copies:
        copy.wait()


def pick_kernel(place_ref, selected_ref, tokens_ref, rows_ref, sel_ref, tile_ref, out_ref, sems):
    g, y, x = whereabouts(place_ref)
    experts, most = selected_ref.shape
    _, tok, width = tile_ref.shape
    first = pltpu.make_async_copy(selected_ref, sel_ref, sems.at[4])
    first.start()
    loads = []
    for c in range(2):
        block = 4 * ((jnp.minimum, jnp.maximum)[c](y, 3 - y)) + x
        at = pl.multiple_of(block * width, width)
        loads.append(
            pltpu.make_async_copy(tokens_ref.at[:, pl.ds(at, width)], tile_ref.at[c], sems.at[c])
        )
        loads[c].start()
    here = experts // 2
    slots = here * most
    first.wait()
    sel = sel_ref[...].astype(F32).astype(BF)
    repeat = one_hot(2 * (iota((slots, experts), 0) // most) + g == iota((slots, experts), 1))
    own = iota((slots, most), 0) % most == iota((slots, most), 1)
    spread = jnp.where(own, dot(repeat, sel), 0.0).astype(BF)
    position = dot(spread, jnp.ones((most, tok), BF))
    named = one_hot(position == iota((slots, tok), 1).astype(F32))
    stores = []
    for c in range(2):
        loads[c].wait()
        rows = jnp.where(position < 0.0, EMPTY, dot(named, tile_ref[c])).astype(BF)
        out_ref[c] = rows.reshape(here, most, width)
        stores.append(pltpu.make_async_copy(out_ref.at[c], rows_ref.at[:, c], sems.at[2 + c]))
        stores[c].start()
    for store in stores:
        store.wait()


def mix_kernel(selected_ref, affinity_ref, mix_ref):
    experts, most = selected_ref.shape
    _, tok, slots = mix_ref.shape
    sel = selected_ref[...].astype(F32).astype(BF)
    tile = one_hot(iota((most, slots), 0) == iota((most, slots), 1) % most)
    mine = iota((experts, slots), 0) == iota((experts, slots), 1) // most

    def as_row(values):
        return jnp.sum(jnp.where(mine, dot(values, tile), 0.0), axis=0, keepdims=True)

    aff = affinity_ref[...]
    high = aff.astype(BF)
    low = (aff - high.astype(F32)).astype(BF)
    hit = as_row(sel) == iota((tok, slots), 0).astype(F32)
    mix_ref[0] = jnp.where(hit, as_row(high), 0.0).astype(BF)
    mix_ref[1] = jnp.where(hit, as_row(low), 0.0).astype(BF)


def compact_kernel(slots_ref, rows_ref, counts_ref):
    blocks, most, width = slots_ref.shape
    cores, lines, peers, part, _ = rows_ref.shape
    slots = blocks * most
    count = cores * part
    data = slots_ref[...].reshape(slots, width)
    live = one_hot(data.astype(F32) < LIMIT)
    first = one_hot(iota((8, width), 1) == 0)
    live_row = lax.dot_general(first, live, (((1,), (1,)), ((), ())), preferred_element_type=F32)
    in_block = one_hot(iota((slots, width), 0) // most == iota((slots, width), 1))
    before = one_hot(iota((width, slots), 0) < iota((width, slots), 1) // most)
    counts = dot(live_row.astype(BF), in_block).astype(BF)
    counts_ref[...] = jnp.broadcast_to(counts[0:1], counts_ref.shape)
    rank = dot(counts, before) + (iota((8, slots), 1) % most).astype(F32)
    rank = jnp.where(live_row > 0.5, rank, -1.0)[0:1]
    take = one_hot(rank == iota((count, slots), 0).astype(F32))
    rows = dot(take, data).astype(BF)
    for c in range(cores):
        for k in range(lines):
            for x in range(peers):
                rows_ref[c, k, x] = rows[c * part : (c + 1) * part]


def seat(block, g):
    y = block // 4
    yy = (0, 1, 1, 0)[y]
    return (y // 2) * 8 + 4 * (yy + g - 2 * yy * g) + block % 4


def ffn_kernel(place_ref, x_ref, *refs):
    *weights, out_ref = refs
    g, _, _ = whereabouts(place_ref)
    peers, _, span = x_ref.shape
    width = peers * span
    x = jnp.concatenate([x_ref[seat(k, g)] for k in range(peers)], axis=1)
    gate = dot(x, jnp.concatenate([w[:width] for w in weights], axis=1))
    up = dot(x, jnp.concatenate([w[width : 2 * width] for w in weights], axis=1))
    hidden = (gate / (1.0 + jnp.exp(-gate)) * up).astype(BF)
    for k in range(0, peers, 2):
        at = 2 * width + k * span
        tiles = [
            jnp.concatenate([w[at + j * span : at + (j + 1) * span] for w in weights], axis=0)
            for j in range(2)
        ]
        partial = dot(hidden, jnp.concatenate(tiles, axis=1)).astype(BF)
        for j in range(2):
            out_ref[seat(k + j, g)] = partial[:, j * span : (j + 1) * span]


def sum_kernel(parts_ref, out_ref):
    cores, lines, peers, part, width = parts_ref.shape
    for c in range(cores):
        total = jnp.zeros((part, width), F32)
        for k in range(lines):
            for x in range(peers):
                total = total + parts_ref[c, k, x].astype(F32)
        out_ref[c * part : (c + 1) * part] = total.astype(BF)


def expand_kernel(rows_ref, counts_ref, out_ref):
    count, width = rows_ref.shape
    blocks, most, _ = out_ref.shape
    slots = blocks * most
    block = iota((slots, width), 0) // most
    place = (iota((slots, width), 0) % most).astype(F32)

    def spread(table):
        dims = (((1,), (1,)), ((), ()))
        return lax.dot_general(table, counts_ref[...], dims, preferred_element_type=F32)

    lanes = iota((slots, width), 1)
    rank = spread(one_hot(lanes < block)) + place
    rank = jnp.where(place < spread(one_hot(lanes == block)), rank, -1.0)
    put = [one_hot(rank - k == lanes.astype(F32)) for k in range(0, count, width)]
    rows = dot(jnp.concatenate(put, axis=1), rows_ref[...]).astype(BF)
    out_ref[...] = rows.reshape(blocks, most, width)


def combine_kernel(mix_ref, rows_ref, out_ref):
    rows = rows_ref[...]
    out_ref[...] = (dot(mix_ref[0], rows) + dot(mix_ref[1], rows)).astype(BF)


def local_call(kernel, outs, *args, place=None, params=(), hbm=(), scratch=()):
    vmem = pl.BlockSpec(memory_space=pltpu.VMEM)
    specs = [pl.BlockSpec()] * len(params) + [vmem] * len(args)
    specs += [pl.BlockSpec(memory_space=pltpu.HBM)] * len(hbm)
    args = [pltpu.with_memory_space_constraint(a, pltpu.VMEM) for a in args]
    args = [*params, *args, *(pltpu.with_memory_space_constraint(a, pltpu.HBM) for a in hbm)]
    if place is not None:
        specs = [pl.BlockSpec(memory_space=pltpu.SMEM)] + specs
        args = [place] + args
    return pl.pallas_call(
        kernel,
        in_specs=specs,
        out_specs=jax.tree.map(
            lambda o: pl.BlockSpec(memory_space=getattr(o, "memory_space", None)), outs
        ),
        out_shape=outs,
        scratch_shapes=scratch,
        compiler_params=pltpu.CompilerParams(vmem_limit_bytes=24 * 2**20),
    )(*args)


def array(shape, dtype=BF):
    return pltpu.VMEM(shape, dtype)


def per_device(tokens, selected, affinity, w_gate, w_up, w_down):
    ep = lax.axis_size(EP)
    layers = lax.axis_size("z")
    team = lax.axis_size(TEAM)
    tok, width = tokens.shape
    experts, most = selected.shape
    span = width // team
    part = ep * most // 4
    lines = lax.axis_size("yy")
    peers = lax.axis_size("x")
    place = lax.axis_index(TP).astype(jnp.int32).reshape(1)
    packed = local_call(
        pack_kernel,
        array((3 * width, span)),
        hbm=(w_gate, w_up, w_down),
        scratch=[pltpu.SemaphoreType.DMA((2 + team,))],
    )
    mine = lax.ppermute(packed, ("c", "g", "yy"), TRADE)
    rows = local_call(
        pick_kernel,
        pltpu.HBM((layers, 2, most, span), BF),
        place=place,
        hbm=(selected, tokens),
        scratch=[
            pltpu.VMEM((experts, most), jnp.int32),
            pltpu.VMEM((2, tok, span), BF),
            pltpu.VMEM((2, layers, most, span), BF),
            pltpu.SemaphoreType.DMA((5,)),
        ],
    )
    arrived = lax.all_to_all(rows.reshape(ep, most, span), EP, 0, 0, tiled=True)
    mix = local_call(
        mix_kernel,
        array((2, tok, experts * most)),
        params=(selected, affinity),
    )
    other = lax.ppermute(mine, "c", CORES)
    copies, counts = local_call(
        compact_kernel, [array((2, lines, peers, part, span)), array((tok, span))], arrived
    )
    chosen = lax.all_to_all(copies.reshape(team, part, span), TEAM, 0, 0, tiled=True)
    counts = lax.ppermute(counts, ("c", "g", "yy"), TRADE)
    chosen, counts = lax.optimization_barrier((chosen, counts))
    partial = local_call(ffn_kernel, array((team, part, span)), chosen, mine, other, place=place)
    summands = lax.all_to_all(partial, TEAM, 0, 0, tiled=True)
    result = local_call(
        sum_kernel, array((2 * part, span)), summands.reshape(2, lines, peers, part, span)
    )
    result = lax.ppermute(result, ("c", "g", "yy"), TRADE)
    result = local_call(expand_kernel, array((ep, most, span)), result, counts)
    returned = lax.all_to_all(result, EP, 0, 0, tiled=True)
    return local_call(
        combine_kernel,
        jax.ShapeDtypeStruct((tok, span), BF),
        mix,
        returned.reshape(experts * most, span),
    )


def solution(mesh):
    torus = Mesh(mesh.devices.reshape(16, 2, 2, 2, 4), ("z", "c", "g", "yy", "x"))
    in_specs = (
        P(EP, None),
        P(None, EP),
        P(None, EP),
        P(EP, None, TP),
        P(EP, None, TP),
        P(EP, TP, None),
    )

    return jax.shard_map(
        per_device, mesh=torus, in_specs=in_specs, out_specs=P(EP, TP), check_vma=False
    )
```

```python
import jax
import jax.numpy as jnp
from jax import lax
from jax.experimental import pallas as pl
from jax.experimental.pallas import tpu as pltpu
from jax.sharding import Mesh
from jax.sharding import PartitionSpec as P

EP = ("z", "c")
TP = ("g", "yy", "x")
TEAM = ("c", "yy", "x")
BF = jnp.bfloat16
F32 = jnp.float32
EMPTY = 64.0
LIMIT = 32.0
TRADE = [(0, 0), (1, 1), (6, 6), (7, 7), (4, 3), (3, 4), (5, 2), (2, 5)]
CORES = [(0, 1), (1, 0)]


def iota(shape, dim):
    return lax.broadcasted_iota(jnp.int32, shape, dim)


def dot(a, b):
    return jnp.dot(a, b, preferred_element_type=F32)


def one_hot(mask):
    return jnp.where(mask, 1.0, 0.0).astype(BF)


def pack_kernel(gate_ref, up_ref, down_ref, out_ref, sems):
    _, width, span = gate_ref.shape
    copies = [(gate_ref.at[0], out_ref.at[:width]), (up_ref.at[0], out_ref.at[width : 2 * width])]
    for k in range(width // span):
        at = 2 * width + k * span
        copies.append((down_ref.at[0, :, k * span : (k + 1) * span], out_ref.at[at : at + span]))
    copies = [pltpu.make_async_copy(*c, sems.at[k]) for k, c in enumerate(copies)]
    for copy in copies:
        copy.start()
    for copy in copies:
        copy.wait()


def pick_kernel(place_ref, selected_ref, tokens_ref, rows_ref, sel_ref, tile_ref, out_ref, sems):
    g = place_ref[0] // 8
    experts, most = selected_ref.shape
    _, tok, width = tile_ref.shape
    first = pltpu.make_async_copy(selected_ref, sel_ref, sems.at[4])
    first.start()
    loads = []
    for c in range(2):
        at = pl.multiple_of((8 * c + place_ref[0] % 8) * width, width)
        loads.append(
            pltpu.make_async_copy(tokens_ref.at[:, pl.ds(at, width)], tile_ref.at[c], sems.at[c])
        )
        loads[c].start()
    here = experts // 2
    slots = here * most
    first.wait()
    sel = sel_ref[...].astype(F32).astype(BF)
    repeat = one_hot(2 * (iota((slots, experts), 0) // most) + g == iota((slots, experts), 1))
    own = iota((slots, most), 0) % most == iota((slots, most), 1)
    spread = jnp.where(own, dot(repeat, sel), 0.0).astype(BF)
    position = dot(spread, jnp.ones((most, tok), BF))
    named = one_hot(position == iota((slots, tok), 1).astype(F32))
    stores = []
    for c in range(2):
        loads[c].wait()
        rows = jnp.where(position < 0.0, EMPTY, dot(named, tile_ref[c])).astype(BF)
        out_ref[c] = rows.reshape(here, most, width)
        stores.append(pltpu.make_async_copy(out_ref.at[c], rows_ref.at[:, c], sems.at[2 + c]))
        stores[c].start()
    for store in stores:
        store.wait()


def mix_kernel(selected_ref, affinity_ref, mix_ref):
    experts, most = selected_ref.shape
    _, _, tok, slots = mix_ref.shape
    part = most // 2
    mine = iota((experts, slots), 0) == iota((experts, slots), 1) // part
    sel = selected_ref[...].astype(F32).astype(BF)
    aff = affinity_ref[...]
    high = aff.astype(BF)
    low = (aff - high.astype(F32)).astype(BF)
    for half in range(2):
        wanted = iota((most, slots), 1) % part + half * part
        tile = one_hot(iota((most, slots), 0) == wanted)

        def as_row(values):
            return jnp.sum(jnp.where(mine, dot(values, tile), 0.0), axis=0, keepdims=True)

        hit = as_row(sel) == iota((tok, slots), 0).astype(F32)
        mix_ref[half, 0] = jnp.where(hit, as_row(high), 0.0).astype(BF)
        mix_ref[half, 1] = jnp.where(hit, as_row(low), 0.0).astype(BF)


def compact_kernel(slots_ref, rows_ref):
    blocks, most, width = slots_ref.shape
    cores, lines, peers, part, _ = rows_ref.shape
    slots = blocks * most
    count = cores * part
    data = slots_ref[...].reshape(slots, width)
    live = one_hot(data.astype(F32) < LIMIT)
    first = one_hot(iota((8, width), 1) == 0)
    live_row = lax.dot_general(first, live, (((1,), (1,)), ((), ())), preferred_element_type=F32)
    in_block = one_hot(iota((slots, blocks), 0) // most == iota((slots, blocks), 1))
    before = one_hot(iota((blocks, slots), 0) < iota((blocks, slots), 1) // most)
    counts = dot(live_row.astype(BF), in_block)
    rank = dot(counts.astype(BF), before) + (iota((8, slots), 1) % most).astype(F32)
    rank = jnp.where(live_row > 0.5, rank, -1.0)[0:1]
    take = one_hot(rank == iota((count, slots), 0).astype(F32))
    rows = dot(take, data).astype(BF)
    for c in range(cores):
        for k in range(lines):
            for x in range(peers):
                rows_ref[c, k, x] = rows[c * part : (c + 1) * part]


def turned(x):
    half = x.shape[1] // 2
    return jnp.concatenate([x[:, half:], x[:, :half]], axis=1)


def joined(left, right):
    return jnp.where(iota(left.shape, 1) < left.shape[1] // 2, left, right)


def ffn_kernel(x_ref, *refs):
    *weights, out_ref = refs
    peers, _, span = x_ref.shape
    width = peers * span
    x = jnp.concatenate([x_ref[k] for k in range(peers)], axis=1)
    gate = dot(x, jnp.concatenate([w[:width] for w in weights], axis=1))
    up = dot(x, jnp.concatenate([w[width : 2 * width] for w in weights], axis=1))
    hidden = (gate / (1.0 + jnp.exp(-gate)) * up).astype(BF)
    half = peers // 2
    for k in range(half):
        tiles = []
        for block in (k, k + half):
            at = 2 * width + block * span
            tiles.append(jnp.concatenate([w[at : at + span] for w in weights], axis=0))
        both = dot(hidden, jnp.concatenate(tiles, axis=1))
        low, high = both[:, :span], both[:, span:]
        out_ref[k] = joined(low, turned(high)).astype(BF)
        out_ref[k + half] = joined(turned(low), high).astype(BF)


def expand_kernel(parts_ref, slots_ref, out_ref):
    cores, lines, peers, part, width = parts_ref.shape
    blocks, most, _ = slots_ref.shape
    slots = blocks * most
    halves = []
    for c in range(cores):
        total = jnp.zeros((part, width), F32)
        for k in range(lines):
            for x in range(peers):
                total = total + parts_ref[c, k, x].astype(F32)
        halves.append(total)
    rows = jnp.concatenate(halves, axis=0)
    rows = jnp.concatenate([rows, turned(rows)], axis=1).astype(BF)
    live = one_hot(slots_ref[...].reshape(slots, width).astype(F32) < LIMIT)
    in_block = one_hot(iota((blocks, slots), 0) == iota((blocks, slots), 1) // most)
    counts = dot(in_block, live).astype(BF)
    few = slots // 2
    step = most // 2
    block = iota((few, blocks), 0) // step
    before = dot(one_hot(iota((few, blocks), 1) < block), counts)
    count = dot(one_hot(iota((few, blocks), 1) == block), counts)
    lanes = iota((few, width), 1).astype(F32)
    found = []
    for half in range(2):
        place = (iota((few, width), 0) % step + half * step).astype(F32)
        rank = jnp.where(place < count, before + place, -1.0)
        put = [one_hot(rank - k == lanes) for k in range(0, cores * part, width)]
        found.append(dot(jnp.concatenate(put, axis=1), rows))
    first, second = found
    for g in range(2):
        straight, swapped = (slice(0, width), slice(width, 2 * width))
        if g == 0:
            out = joined(first[:, straight], second[:, swapped])
        else:
            out = joined(first[:, swapped], second[:, straight])
        out_ref[:, g] = out.astype(BF).reshape(blocks, step, width)


def combine_kernel(mix_ref, rows_ref, out_ref):
    layers, cores, teams, step, width = rows_ref.shape
    both = [rows_ref[:, c].reshape(layers * teams * step, width) for c in range(cores)]
    both = jnp.concatenate(both, axis=1)
    first = dot(mix_ref[0, 0], both) + dot(mix_ref[0, 1], both)
    second = dot(mix_ref[1, 0], both) + dot(mix_ref[1, 1], both)
    low = first[:, :width] + turned(second[:, :width])
    high = turned(first[:, width:]) + second[:, width:]
    out_ref[...] = joined(low, high).astype(BF)


def local_call(kernel, outs, *args, place=None, params=(), hbm=(), scratch=()):
    vmem = pl.BlockSpec(memory_space=pltpu.VMEM)
    specs = [pl.BlockSpec()] * len(params) + [vmem] * len(args)
    specs += [pl.BlockSpec(memory_space=pltpu.HBM)] * len(hbm)
    args = [pltpu.with_memory_space_constraint(a, pltpu.VMEM) for a in args]
    args = [*params, *args, *(pltpu.with_memory_space_constraint(a, pltpu.HBM) for a in hbm)]
    if place is not None:
        specs = [pl.BlockSpec(memory_space=pltpu.SMEM)] + specs
        args = [place] + args
    return pl.pallas_call(
        kernel,
        in_specs=specs,
        out_specs=jax.tree.map(
            lambda o: pl.BlockSpec(memory_space=getattr(o, "memory_space", None)), outs
        ),
        out_shape=outs,
        scratch_shapes=scratch,
        compiler_params=pltpu.CompilerParams(vmem_limit_bytes=24 * 2**20),
    )(*args)


def array(shape, dtype=BF):
    return pltpu.VMEM(shape, dtype)


def per_device(tokens, selected, affinity, w_gate, w_up, w_down):
    ep = lax.axis_size(EP)
    layers = lax.axis_size("z")
    team = lax.axis_size(TEAM)
    tok, width = tokens.shape
    experts, most = selected.shape
    span = width // team
    part = ep * most // 4
    lines = lax.axis_size("yy")
    peers = lax.axis_size("x")
    place = lax.axis_index(TP).astype(jnp.int32).reshape(1)
    packed = local_call(
        pack_kernel,
        array((3 * width, span)),
        hbm=(w_gate, w_up, w_down),
        scratch=[pltpu.SemaphoreType.DMA((2 + team,))],
    )
    mine = lax.ppermute(packed, ("c", "g", "yy"), TRADE)
    rows = local_call(
        pick_kernel,
        pltpu.HBM((layers, 2, most, span), BF),
        place=place,
        hbm=(selected, tokens),
        scratch=[
            pltpu.VMEM((experts, most), jnp.int32),
            pltpu.VMEM((2, tok, span), BF),
            pltpu.VMEM((2, layers, most, span), BF),
            pltpu.SemaphoreType.DMA((5,)),
        ],
    )
    arrived = lax.all_to_all(rows.reshape(ep, most, span), EP, 0, 0, tiled=True)
    mix = local_call(
        mix_kernel,
        array((2, 2, tok, experts * most // 2)),
        params=(selected, affinity),
    )
    other = lax.ppermute(mine, "c", CORES)
    copies = local_call(compact_kernel, array((2, lines, peers, part, span)), arrived)
    chosen = lax.all_to_all(copies.reshape(team, part, span), TEAM, 0, 0, tiled=True)
    partial = local_call(
        ffn_kernel,
        array((team, part, span)),
        chosen,
        mine,
        other,
    )
    summands = lax.all_to_all(partial, TEAM, 0, 0, tiled=True)
    result = local_call(
        expand_kernel,
        array((ep, 2, most // 2, span)),
        summands.reshape(2, lines, peers, part, span),
        arrived,
    )
    returned = lax.all_to_all(
        result.reshape(2 * ep, most // 2, span), ("z", "c", "g"), 0, 0, tiled=True
    )
    return local_call(
        combine_kernel,
        jax.ShapeDtypeStruct((tok, span), BF),
        mix,
        returned.reshape(layers, 2, 2, most // 2, span),
    )


def solution(mesh):
    torus = Mesh(mesh.devices.reshape(16, 2, 2, 2, 4), ("z", "c", "g", "yy", "x"))
    in_specs = (
        P(EP, None),
        P(None, EP),
        P(None, EP),
        P(EP, None, TP),
        P(EP, None, TP),
        P(EP, TP, None),
    )

    return jax.shard_map(
        per_device, mesh=torus, in_specs=in_specs, out_specs=P(EP, TP), check_vma=False
    )
```

```python
import jax
import jax.numpy as jnp
from jax import lax
from jax.experimental import pallas as pl
from jax.experimental.pallas import tpu as pltpu
from jax.sharding import Mesh
from jax.sharding import PartitionSpec as P

EP = ("z", "c")
TP = ("g", "yy", "x")
TEAM = ("c", "yy", "x")
BF = jnp.bfloat16
F32 = jnp.float32
EMPTY = 64.0
LIMIT = 32.0
TRADE = [(0, 0), (1, 1), (6, 6), (7, 7), (4, 3), (3, 4), (5, 2), (2, 5)]
CORES = [(0, 1), (1, 0)]


def iota(shape, dim):
    return lax.broadcasted_iota(jnp.int32, shape, dim)


def dot(a, b):
    return jnp.dot(a, b, preferred_element_type=F32)


def one_hot(mask):
    return jnp.where(mask, 1.0, 0.0).astype(BF)


def pack_kernel(gate_ref, up_ref, down_ref, out_ref, rest_ref, down_out_ref, sems):
    _, width, span = gate_ref.shape
    copies = [(gate_ref.at[0], out_ref.at[:width]), (up_ref.at[0], out_ref.at[width:])]
    for at in range(0, width, span):
        copies.append((down_ref.at[0, :, at : at + span], down_out_ref.at[at : at + span]))
    copies = [pltpu.make_async_copy(*c, sems.at[k]) for k, c in enumerate(copies)]
    for copy in copies:
        copy.start()
    for copy in copies:
        copy.wait()
    store = pltpu.make_async_copy(down_out_ref, rest_ref, sems.at[0])
    store.start()
    store.wait()


def pick_kernel(place_ref, selected_ref, tokens_ref, rows_ref, sel_ref, tile_ref, out_ref, sems):
    g = place_ref[0] // 8
    experts, most = selected_ref.shape
    _, tok, width = tile_ref.shape
    first = pltpu.make_async_copy(selected_ref, sel_ref, sems.at[4])
    first.start()
    loads = []
    for c in range(2):
        at = pl.multiple_of((8 * c + place_ref[0] % 8) * width, width)
        loads.append(
            pltpu.make_async_copy(tokens_ref.at[:, pl.ds(at, width)], tile_ref.at[c], sems.at[c])
        )
        loads[c].start()
    here = experts // 2
    slots = here * most
    first.wait()
    sel = sel_ref[...].astype(F32).astype(BF)
    repeat = one_hot(2 * (iota((slots, experts), 0) // most) + g == iota((slots, experts), 1))
    own = iota((slots, most), 0) % most == iota((slots, most), 1)
    spread = jnp.where(own, dot(repeat, sel), 0.0).astype(BF)
    position = dot(spread, jnp.ones((most, tok), BF))
    named = one_hot(position == iota((slots, tok), 1).astype(F32))
    stores = []
    for c in range(2):
        loads[c].wait()
        rows = jnp.where(position < 0.0, EMPTY, dot(named, tile_ref[c])).astype(BF)
        out_ref[c] = rows.reshape(here, most, width)
        stores.append(pltpu.make_async_copy(out_ref.at[c], rows_ref.at[:, c], sems.at[2 + c]))
        stores[c].start()
    for store in stores:
        store.wait()


def mix_kernel(selected_ref, affinity_ref, out_ref, mix_ref, sem):
    experts, most = selected_ref.shape
    _, _, tok, slots = mix_ref.shape
    part = most // 2
    mine = iota((experts, slots), 0) == iota((experts, slots), 1) // part
    sel = selected_ref[...].astype(F32).astype(BF)
    aff = affinity_ref[...]
    high = aff.astype(BF)
    low = (aff - high.astype(F32)).astype(BF)
    for half in range(2):
        wanted = iota((most, slots), 1) % part + half * part
        tile = one_hot(iota((most, slots), 0) == wanted)

        def as_row(values):
            return jnp.sum(jnp.where(mine, dot(values, tile), 0.0), axis=0, keepdims=True)

        hit = as_row(sel) == iota((tok, slots), 0).astype(F32)
        mix_ref[half, 0] = jnp.where(hit, as_row(high), 0.0).astype(BF)
        mix_ref[half, 1] = jnp.where(hit, as_row(low), 0.0).astype(BF)
    store = pltpu.make_async_copy(mix_ref, out_ref, sem)
    store.start()
    store.wait()


def compact_kernel(slots_ref, rows_ref):
    blocks, most, width = slots_ref.shape
    cores, lines, peers, part, _ = rows_ref.shape
    slots = blocks * most
    count = cores * part
    data = slots_ref[...].reshape(slots, width)
    live = one_hot(data.astype(F32) < LIMIT)
    first = one_hot(iota((8, width), 1) == 0)
    live_row = lax.dot_general(first, live, (((1,), (1,)), ((), ())), preferred_element_type=F32)
    in_block = one_hot(iota((slots, blocks), 0) // most == iota((slots, blocks), 1))
    before = one_hot(iota((blocks, slots), 0) < iota((blocks, slots), 1) // most)
    counts = dot(live_row.astype(BF), in_block)
    rank = dot(counts.astype(BF), before) + (iota((8, slots), 1) % most).astype(F32)
    rank = jnp.where(live_row > 0.5, rank, -1.0)[0:1]
    take = one_hot(rank == iota((count, slots), 0).astype(F32))
    rows = dot(take, data).astype(BF)
    for c in range(cores):
        for k in range(lines):
            for x in range(peers):
                rows_ref[c, k, x] = rows[c * part : (c + 1) * part]


def turned(x):
    half = x.shape[1] // 2
    return jnp.concatenate([x[:, half:], x[:, :half]], axis=1)


def joined(left, right):
    return jnp.where(iota(left.shape, 1) < left.shape[1] // 2, left, right)


def ffn_kernel(x_ref, mine_ref, other_ref, mine_down_ref, other_down_ref, out_ref, down_ref, sems):
    peers, _, span = x_ref.shape
    width = peers * span
    loads = []
    for k, ref in enumerate((mine_down_ref, other_down_ref)):
        loads.append(pltpu.make_async_copy(ref, down_ref.at[k], sems.at[k]))
        loads[k].start()
    x = jnp.concatenate([x_ref[k] for k in range(peers)], axis=1)
    pair = (mine_ref, other_ref)
    gate = dot(x, jnp.concatenate([w[:width] for w in pair], axis=1))
    up = dot(x, jnp.concatenate([w[width:] for w in pair], axis=1))
    hidden = (gate / (1.0 + jnp.exp(-gate)) * up).astype(BF)
    for load in loads:
        load.wait()
    half = peers // 2
    for k in range(half):
        tiles = []
        for at in (k * span, (k + half) * span):
            tiles.append(jnp.concatenate([down_ref[j, at : at + span] for j in range(2)], axis=0))
        both = dot(hidden, jnp.concatenate(tiles, axis=1))
        low, high = both[:, :span], both[:, span:]
        out_ref[k] = joined(low, turned(high)).astype(BF)
        out_ref[k + half] = joined(turned(low), high).astype(BF)


def expand_kernel(parts_ref, slots_ref, out_ref):
    cores, lines, peers, part, width = parts_ref.shape
    blocks, most, _ = slots_ref.shape
    slots = blocks * most
    halves = []
    for c in range(cores):
        total = jnp.zeros((part, width), F32)
        for k in range(lines):
            for x in range(peers):
                total = total + parts_ref[c, k, x].astype(F32)
        halves.append(total)
    rows = jnp.concatenate(halves, axis=0)
    rows = jnp.concatenate([rows, turned(rows)], axis=1).astype(BF)
    live = one_hot(slots_ref[...].reshape(slots, width).astype(F32) < LIMIT)
    in_block = one_hot(iota((blocks, slots), 0) == iota((blocks, slots), 1) // most)
    counts = dot(in_block, live).astype(BF)
    few = slots // 2
    step = most // 2
    block = iota((few, blocks), 0) // step
    before = dot(one_hot(iota((few, blocks), 1) < block), counts)
    count = dot(one_hot(iota((few, blocks), 1) == block), counts)
    lanes = iota((few, width), 1).astype(F32)
    found = []
    for half in range(2):
        place = (iota((few, width), 0) % step + half * step).astype(F32)
        rank = jnp.where(place < count, before + place, -1.0)
        put = [one_hot(rank - k == lanes) for k in range(0, cores * part, width)]
        found.append(dot(jnp.concatenate(put, axis=1), rows))
    first, second = found
    for g in range(2):
        straight, swapped = (slice(0, width), slice(width, 2 * width))
        if g == 0:
            out = joined(first[:, straight], second[:, swapped])
        else:
            out = joined(first[:, swapped], second[:, straight])
        out_ref[:, g] = out.astype(BF).reshape(blocks, step, width)


def combine_kernel(mix_ref, rows_ref, out_ref):
    layers, cores, teams, step, width = rows_ref.shape
    both = [rows_ref[:, c].reshape(layers * teams * step, width) for c in range(cores)]
    both = jnp.concatenate(both, axis=1)
    first = dot(mix_ref[0, 0], both) + dot(mix_ref[0, 1], both)
    second = dot(mix_ref[1, 0], both) + dot(mix_ref[1, 1], both)
    low = first[:, :width] + turned(second[:, :width])
    high = turned(first[:, width:]) + second[:, width:]
    out_ref[...] = joined(low, high).astype(BF)


def local_call(kernel, outs, *args, place=None, params=(), hbm=(), scratch=()):
    vmem = pl.BlockSpec(memory_space=pltpu.VMEM)
    specs = [pl.BlockSpec()] * len(params) + [vmem] * len(args)
    specs += [pl.BlockSpec(memory_space=pltpu.HBM)] * len(hbm)
    args = [pltpu.with_memory_space_constraint(a, pltpu.VMEM) for a in args]
    args = [*params, *args, *(pltpu.with_memory_space_constraint(a, pltpu.HBM) for a in hbm)]
    if place is not None:
        specs = [pl.BlockSpec(memory_space=pltpu.SMEM)] + specs
        args = [place] + args
    return pl.pallas_call(
        kernel,
        in_specs=specs,
        out_specs=jax.tree.map(
            lambda o: pl.BlockSpec(memory_space=getattr(o, "memory_space", None)), outs
        ),
        out_shape=outs,
        scratch_shapes=scratch,
        compiler_params=pltpu.CompilerParams(vmem_limit_bytes=24 * 2**20),
    )(*args)


def array(shape, dtype=BF):
    return pltpu.VMEM(shape, dtype)


def per_device(tokens, selected, affinity, w_gate, w_up, w_down):
    ep = lax.axis_size(EP)
    layers = lax.axis_size("z")
    team = lax.axis_size(TEAM)
    tok, width = tokens.shape
    experts, most = selected.shape
    span = width // team
    part = ep * most // 4
    lines = lax.axis_size("yy")
    peers = lax.axis_size("x")
    place = lax.axis_index(TP).astype(jnp.int32).reshape(1)
    packed, rest = local_call(
        pack_kernel,
        [array((2 * width, span)), pltpu.HBM((width, span), BF)],
        hbm=(w_gate, w_up, w_down),
        scratch=[pltpu.VMEM((width, span), BF), pltpu.SemaphoreType.DMA((2 + team,))],
    )
    mine = lax.ppermute(packed, ("c", "g", "yy"), TRADE)
    mine_down = lax.ppermute(rest, ("c", "g", "yy"), TRADE)
    rows = local_call(
        pick_kernel,
        pltpu.HBM((layers, 2, most, span), BF),
        place=place,
        hbm=(selected, tokens),
        scratch=[
            pltpu.VMEM((experts, most), jnp.int32),
            pltpu.VMEM((2, tok, span), BF),
            pltpu.VMEM((2, layers, most, span), BF),
            pltpu.SemaphoreType.DMA((5,)),
        ],
    )
    arrived = lax.all_to_all(rows.reshape(ep, most, span), EP, 0, 0, tiled=True)
    mix = local_call(
        mix_kernel,
        pltpu.HBM((2, 2, tok, experts * most // 2), BF),
        params=(selected, affinity),
        scratch=[
            pltpu.VMEM((2, 2, tok, experts * most // 2), BF),
            pltpu.SemaphoreType.DMA(()),
        ],
    )
    other = lax.ppermute(mine, "c", CORES)
    other_down = lax.ppermute(mine_down, "c", CORES)
    copies = local_call(compact_kernel, array((2, lines, peers, part, span)), arrived)
    chosen = lax.all_to_all(copies.reshape(team, part, span), TEAM, 0, 0, tiled=True)
    partial = local_call(
        ffn_kernel,
        array((team, part, span)),
        chosen,
        mine,
        other,
        hbm=(mine_down, other_down),
        scratch=[pltpu.VMEM((2, width, span), BF), pltpu.SemaphoreType.DMA((2,))],
    )
    summands = lax.all_to_all(partial, TEAM, 0, 0, tiled=True)
    result = local_call(
        expand_kernel,
        array((ep, 2, most // 2, span)),
        summands.reshape(2, lines, peers, part, span),
        arrived,
    )
    returned = lax.all_to_all(
        result.reshape(2 * ep, most // 2, span), ("z", "c", "g"), 0, 0, tiled=True
    )
    return local_call(
        combine_kernel,
        jax.ShapeDtypeStruct((tok, span), BF),
        mix,
        returned.reshape(layers, 2, 2, most // 2, span),
    )


def solution(mesh):
    torus = Mesh(mesh.devices.reshape(16, 2, 2, 2, 4), ("z", "c", "g", "yy", "x"))
    in_specs = (
        P(EP, None),
        P(None, EP),
        P(None, EP),
        P(EP, None, TP),
        P(EP, None, TP),
        P(EP, TP, None),
    )

    return jax.shard_map(
        per_device, mesh=torus, in_specs=in_specs, out_specs=P(EP, TP), check_vma=False
    )
```

```python
import jax
import jax.numpy as jnp
from jax import lax
from jax.experimental import pallas as pl
from jax.experimental.pallas import tpu as pltpu
from jax.sharding import Mesh
from jax.sharding import PartitionSpec as P

EP = ("z", "c")
TP = ("g", "yy", "x")
TEAM = ("c", "yy", "x")
BF = jnp.bfloat16
F32 = jnp.float32
EMPTY = 64.0
LIMIT = 32.0
TRADE = [(0, 0), (1, 1), (6, 6), (7, 7), (4, 3), (3, 4), (5, 2), (2, 5)]
CORES = [(0, 1), (1, 0)]


def turned_groups(layers, members):
    ranks = layers * members
    return [[(k + ranks // 2) % ranks for k in range(ranks)]]


def iota(shape, dim):
    return lax.broadcasted_iota(jnp.int32, shape, dim)


def dot(a, b):
    return jnp.dot(a, b, preferred_element_type=F32)


def one_hot(mask):
    return jnp.where(mask, 1.0, 0.0).astype(BF)


def pack_kernel(gate_ref, up_ref, down_ref, out_ref, sems):
    _, width, span = gate_ref.shape
    copies = [(gate_ref.at[0], out_ref.at[:width]), (up_ref.at[0], out_ref.at[width : 2 * width])]
    for k in range(width // span):
        at = 2 * width + k * span
        copies.append((down_ref.at[0, :, k * span : (k + 1) * span], out_ref.at[at : at + span]))
    copies = [pltpu.make_async_copy(*c, sems.at[k]) for k, c in enumerate(copies)]
    for copy in copies:
        copy.start()
    for copy in copies:
        copy.wait()


def pick_kernel(place_ref, selected_ref, tokens_ref, rows_ref, sel_ref, tile_ref, out_ref, sems):
    g = place_ref[0] // 8
    experts, most = selected_ref.shape
    _, tok, width = tile_ref.shape
    first = pltpu.make_async_copy(selected_ref, sel_ref, sems.at[4])
    first.start()
    loads = []
    for c in range(2):
        at = pl.multiple_of((8 * c + place_ref[0] % 8) * width, width)
        loads.append(
            pltpu.make_async_copy(tokens_ref.at[:, pl.ds(at, width)], tile_ref.at[c], sems.at[c])
        )
        loads[c].start()
    here = experts // 2
    slots = here * most
    first.wait()
    sel = sel_ref[...].astype(F32).astype(BF)
    layer = (iota((slots, experts), 0) // most + here // 2) % here
    repeat = one_hot(2 * layer + g == iota((slots, experts), 1))
    own = iota((slots, most), 0) % most == iota((slots, most), 1)
    spread = jnp.where(own, dot(repeat, sel), 0.0).astype(BF)
    position = dot(spread, jnp.ones((most, tok), BF))
    named = one_hot(position == iota((slots, tok), 1).astype(F32))
    stores = []
    for c in range(2):
        loads[c].wait()
        rows = jnp.where(position < 0.0, EMPTY, dot(named, tile_ref[c])).astype(BF)
        out_ref[c] = rows.reshape(here, most, width)
        stores.append(pltpu.make_async_copy(out_ref.at[c], rows_ref.at[:, c], sems.at[2 + c]))
        stores[c].start()
    for store in stores:
        store.wait()


def mix_kernel(selected_ref, affinity_ref, mix_ref):
    experts, most = selected_ref.shape
    _, _, tok, slots = mix_ref.shape
    part = most // 2
    expert = (iota((experts, slots), 1) // part + experts // 2) % experts
    mine = iota((experts, slots), 0) == expert
    sel = selected_ref[...].astype(F32).astype(BF)
    aff = affinity_ref[...]
    high = aff.astype(BF)
    low = (aff - high.astype(F32)).astype(BF)
    for half in range(2):
        wanted = iota((most, slots), 1) % part + half * part
        tile = one_hot(iota((most, slots), 0) == wanted)

        def as_row(values):
            return jnp.sum(jnp.where(mine, dot(values, tile), 0.0), axis=0, keepdims=True)

        hit = as_row(sel) == iota((tok, slots), 0).astype(F32)
        mix_ref[half, 0] = jnp.where(hit, as_row(high), 0.0).astype(BF)
        mix_ref[half, 1] = jnp.where(hit, as_row(low), 0.0).astype(BF)


def compact_kernel(slots_ref, rows_ref):
    blocks, most, width = slots_ref.shape
    cores, lines, peers, part, _ = rows_ref.shape
    slots = blocks * most
    count = cores * part
    data = slots_ref[...].reshape(slots, width)
    live = one_hot(data.astype(F32) < LIMIT)
    first = one_hot(iota((8, width), 1) == 0)
    live_row = lax.dot_general(first, live, (((1,), (1,)), ((), ())), preferred_element_type=F32)
    in_block = one_hot(iota((slots, blocks), 0) // most == iota((slots, blocks), 1))
    before = one_hot(iota((blocks, slots), 0) < iota((blocks, slots), 1) // most)
    counts = dot(live_row.astype(BF), in_block)
    rank = dot(counts.astype(BF), before) + (iota((8, slots), 1) % most).astype(F32)
    rank = jnp.where(live_row > 0.5, rank, -1.0)[0:1]
    take = one_hot(rank == iota((count, slots), 0).astype(F32))
    rows = dot(take, data).astype(BF)
    for c in range(cores):
        for k in range(lines):
            for x in range(peers):
                rows_ref[c, k, x] = rows[c * part : (c + 1) * part]


def turned(x):
    half = x.shape[1] // 2
    return jnp.concatenate([x[:, half:], x[:, :half]], axis=1)


def joined(left, right):
    return jnp.where(iota(left.shape, 1) < left.shape[1] // 2, left, right)


def ffn_kernel(x_ref, *refs):
    *weights, out_ref = refs
    peers, _, span = x_ref.shape
    width = peers * span
    x = jnp.concatenate([x_ref[k] for k in range(peers)], axis=1)
    gate = dot(x, jnp.concatenate([w[:width] for w in weights], axis=1))
    up = dot(x, jnp.concatenate([w[width : 2 * width] for w in weights], axis=1))
    hidden = (gate / (1.0 + jnp.exp(-gate)) * up).astype(BF)
    half = peers // 2
    for k in range(half):
        tiles = []
        for block in (k, k + half):
            at = 2 * width + block * span
            tiles.append(jnp.concatenate([w[at : at + span] for w in weights], axis=0))
        both = dot(hidden, jnp.concatenate(tiles, axis=1))
        low, high = both[:, :span], both[:, span:]
        out_ref[k] = joined(low, turned(high)).astype(BF)
        out_ref[k + half] = joined(turned(low), high).astype(BF)


def expand_kernel(parts_ref, slots_ref, out_ref):
    cores, lines, peers, part, width = parts_ref.shape
    blocks, most, _ = slots_ref.shape
    slots = blocks * most
    halves = []
    for c in range(cores):
        total = jnp.zeros((part, width), F32)
        for k in range(lines):
            for x in range(peers):
                total = total + parts_ref[c, k, x].astype(F32)
        halves.append(total)
    rows = jnp.concatenate(halves, axis=0)
    rows = jnp.concatenate([rows, turned(rows)], axis=1).astype(BF)
    live = one_hot(slots_ref[...].reshape(slots, width).astype(F32) < LIMIT)
    in_block = one_hot(iota((blocks, slots), 0) == iota((blocks, slots), 1) // most)
    counts = dot(in_block, live).astype(BF)
    few = slots // 2
    step = most // 2
    block = iota((few, blocks), 0) // step
    before = dot(one_hot(iota((few, blocks), 1) < block), counts)
    count = dot(one_hot(iota((few, blocks), 1) == block), counts)
    lanes = iota((few, width), 1).astype(F32)
    found = []
    for half in range(2):
        place = (iota((few, width), 0) % step + half * step).astype(F32)
        rank = jnp.where(place < count, before + place, -1.0)
        put = [one_hot(rank - k == lanes) for k in range(0, cores * part, width)]
        found.append(dot(jnp.concatenate(put, axis=1), rows))
    first, second = found
    for g in range(2):
        straight, swapped = (slice(0, width), slice(width, 2 * width))
        if g == 0:
            out = joined(first[:, straight], second[:, swapped])
        else:
            out = joined(first[:, swapped], second[:, straight])
        out_ref[:, g] = out.astype(BF).reshape(blocks, step, width)


def combine_kernel(mix_ref, rows_ref, out_ref):
    layers, cores, teams, step, width = rows_ref.shape
    both = [rows_ref[:, c].reshape(layers * teams * step, width) for c in range(cores)]
    both = jnp.concatenate(both, axis=1)
    first = dot(mix_ref[0, 0], both) + dot(mix_ref[0, 1], both)
    second = dot(mix_ref[1, 0], both) + dot(mix_ref[1, 1], both)
    low = first[:, :width] + turned(second[:, :width])
    high = turned(first[:, width:]) + second[:, width:]
    out_ref[...] = joined(low, high).astype(BF)


def local_call(kernel, outs, *args, place=None, params=(), hbm=(), scratch=()):
    vmem = pl.BlockSpec(memory_space=pltpu.VMEM)
    specs = [pl.BlockSpec()] * len(params) + [vmem] * len(args)
    specs += [pl.BlockSpec(memory_space=pltpu.HBM)] * len(hbm)
    args = [pltpu.with_memory_space_constraint(a, pltpu.VMEM) for a in args]
    args = [*params, *args, *(pltpu.with_memory_space_constraint(a, pltpu.HBM) for a in hbm)]
    if place is not None:
        specs = [pl.BlockSpec(memory_space=pltpu.SMEM)] + specs
        args = [place] + args
    return pl.pallas_call(
        kernel,
        in_specs=specs,
        out_specs=jax.tree.map(
            lambda o: pl.BlockSpec(memory_space=getattr(o, "memory_space", None)), outs
        ),
        out_shape=outs,
        scratch_shapes=scratch,
        compiler_params=pltpu.CompilerParams(vmem_limit_bytes=24 * 2**20),
    )(*args)


def array(shape, dtype=BF):
    return pltpu.VMEM(shape, dtype)


def per_device(tokens, selected, affinity, w_gate, w_up, w_down):
    ep = lax.axis_size(EP)
    layers = lax.axis_size("z")
    team = lax.axis_size(TEAM)
    tok, width = tokens.shape
    experts, most = selected.shape
    span = width // team
    part = ep * most // 4
    lines = lax.axis_size("yy")
    peers = lax.axis_size("x")
    place = lax.axis_index(TP).astype(jnp.int32).reshape(1)
    packed = local_call(
        pack_kernel,
        array((3 * width, span)),
        hbm=(w_gate, w_up, w_down),
        scratch=[pltpu.SemaphoreType.DMA((2 + team,))],
    )
    mine = lax.ppermute(packed, ("c", "g", "yy"), TRADE)
    rows = local_call(
        pick_kernel,
        pltpu.HBM((layers, 2, most, span), BF),
        place=place,
        hbm=(selected, tokens),
        scratch=[
            pltpu.VMEM((experts, most), jnp.int32),
            pltpu.VMEM((2, tok, span), BF),
            pltpu.VMEM((2, layers, most, span), BF),
            pltpu.SemaphoreType.DMA((5,)),
        ],
    )
    arrived = lax.all_to_all(
        rows.reshape(ep, most, span),
        EP,
        0,
        0,
        axis_index_groups=turned_groups(layers, 2),
        tiled=True,
    )
    mix = local_call(
        mix_kernel,
        array((2, 2, tok, experts * most // 2)),
        params=(selected, affinity),
    )
    other = lax.ppermute(mine, "c", CORES)
    copies = local_call(compact_kernel, array((2, lines, peers, part, span)), arrived)
    chosen = lax.all_to_all(copies.reshape(team, part, span), TEAM, 0, 0, tiled=True)
    partial = local_call(
        ffn_kernel,
        array((team, part, span)),
        chosen,
        mine,
        other,
    )
    summands = lax.all_to_all(partial, TEAM, 0, 0, tiled=True)
    result = local_call(
        expand_kernel,
        array((ep, 2, most // 2, span)),
        summands.reshape(2, lines, peers, part, span),
        arrived,
    )
    returned = lax.all_to_all(
        result.reshape(2 * ep, most // 2, span),
        ("z", "c", "g"),
        0,
        0,
        axis_index_groups=turned_groups(layers, 4),
        tiled=True,
    )
    return local_call(
        combine_kernel,
        jax.ShapeDtypeStruct((tok, span), BF),
        mix,
        returned.reshape(layers, 2, 2, most // 2, span),
    )


def solution(mesh):
    torus = Mesh(mesh.devices.reshape(16, 2, 2, 2, 4), ("z", "c", "g", "yy", "x"))
    in_specs = (
        P(EP, None),
        P(None, EP),
        P(None, EP),
        P(EP, None, TP),
        P(EP, None, TP),
        P(EP, TP, None),
    )

    return jax.shard_map(
        per_device, mesh=torus, in_specs=in_specs, out_specs=P(EP, TP), check_vma=False
    )
```

```python
import jax
import jax.numpy as jnp
from jax import lax
from jax.experimental import pallas as pl
from jax.experimental.pallas import tpu as pltpu
from jax.sharding import Mesh
from jax.sharding import PartitionSpec as P

EP = ("z", "c")
TP = ("g", "yy", "x")
TEAM = ("c", "yy", "x")
BF = jnp.bfloat16
F32 = jnp.float32
EMPTY = 64.0
LIMIT = 32.0
TRADE = [(0, 0), (1, 1), (6, 6), (7, 7), (4, 3), (3, 4), (5, 2), (2, 5)]
CORES = [(0, 1), (1, 0)]


def turned_groups(layers, teams):
    order = [(p + layers // 2) % layers for p in range(layers)]
    return [[(z * 2 + c) * teams + g for z in order for c in (1, 0) for g in range(teams)]]


def team_groups(members):
    return [[(k + members // 2) % members for k in range(members)]]


def iota(shape, dim):
    return lax.broadcasted_iota(jnp.int32, shape, dim)


def dot(a, b):
    return jnp.dot(a, b, preferred_element_type=F32)


def one_hot(mask):
    return jnp.where(mask, 1.0, 0.0).astype(BF)


def pack_kernel(gate_ref, up_ref, down_ref, out_ref, sems):
    _, width, span = gate_ref.shape
    copies = [(gate_ref.at[0], out_ref.at[:width]), (up_ref.at[0], out_ref.at[width : 2 * width])]
    for k in range(width // span):
        at = 2 * width + k * span
        copies.append((down_ref.at[0, :, k * span : (k + 1) * span], out_ref.at[at : at + span]))
    copies = [pltpu.make_async_copy(*c, sems.at[k]) for k, c in enumerate(copies)]
    for copy in copies:
        copy.start()
    for copy in copies:
        copy.wait()


def pick_kernel(place_ref, selected_ref, tokens_ref, rows_ref, sel_ref, tile_ref, out_ref, sems):
    g = place_ref[0] // 8
    experts, most = selected_ref.shape
    _, tok, width = tile_ref.shape
    first = pltpu.make_async_copy(selected_ref, sel_ref, sems.at[4])
    first.start()
    loads = []
    for c in range(2):
        at = pl.multiple_of((8 * (1 - c) + place_ref[0] % 8) * width, width)
        loads.append(
            pltpu.make_async_copy(tokens_ref.at[:, pl.ds(at, width)], tile_ref.at[c], sems.at[c])
        )
        loads[c].start()
    here = experts // 2
    slots = here * most
    first.wait()
    sel = sel_ref[...].astype(F32).astype(BF)
    layer = (iota((slots, experts), 0) // most + here // 2) % here
    repeat = one_hot(2 * layer + g == iota((slots, experts), 1))
    own = iota((slots, most), 0) % most == iota((slots, most), 1)
    spread = jnp.where(own, dot(repeat, sel), 0.0).astype(BF)
    position = dot(spread, jnp.ones((most, tok), BF))
    named = one_hot(position == iota((slots, tok), 1).astype(F32))
    stores = []
    for c in range(2):
        loads[c].wait()
        rows = jnp.where(position < 0.0, EMPTY, dot(named, tile_ref[c])).astype(BF)
        out_ref[c] = rows.reshape(here, most, width)
        stores.append(pltpu.make_async_copy(out_ref.at[c], rows_ref.at[:, c], sems.at[2 + c]))
        stores[c].start()
    for store in stores:
        store.wait()


def mix_kernel(selected_ref, affinity_ref, mix_ref):
    experts, most = selected_ref.shape
    _, _, tok, slots = mix_ref.shape
    part = most // 2
    expert = (iota((experts, slots), 1) // part + experts // 2) % experts
    mine = iota((experts, slots), 0) == expert
    sel = selected_ref[...].astype(F32).astype(BF)
    aff = affinity_ref[...]
    high = aff.astype(BF)
    low = (aff - high.astype(F32)).astype(BF)
    for half in range(2):
        wanted = iota((most, slots), 1) % part + half * part
        tile = one_hot(iota((most, slots), 0) == wanted)

        def as_row(values):
            return jnp.sum(jnp.where(mine, dot(values, tile), 0.0), axis=0, keepdims=True)

        hit = as_row(sel) == iota((tok, slots), 0).astype(F32)
        mix_ref[half, 0] = jnp.where(hit, as_row(high), 0.0).astype(BF)
        mix_ref[half, 1] = jnp.where(hit, as_row(low), 0.0).astype(BF)


def compact_kernel(slots_ref, rows_ref):
    blocks, most, width = slots_ref.shape
    cores, lines, peers, part, _ = rows_ref.shape
    slots = blocks * most
    count = cores * part
    data = slots_ref[...].reshape(slots, width)
    live = one_hot(data.astype(F32) < LIMIT)
    first = one_hot(iota((8, width), 1) == 0)
    live_row = lax.dot_general(first, live, (((1,), (1,)), ((), ())), preferred_element_type=F32)
    in_block = one_hot(iota((slots, blocks), 0) // most == iota((slots, blocks), 1))
    before = one_hot(iota((blocks, slots), 0) < iota((blocks, slots), 1) // most)
    counts = dot(live_row.astype(BF), in_block)
    rank = dot(counts.astype(BF), before) + (iota((8, slots), 1) % most).astype(F32)
    rank = jnp.where(live_row > 0.5, rank, -1.0)[0:1]
    take = one_hot(rank == iota((count, slots), 0).astype(F32))
    rows = dot(take, data).astype(BF)
    for c in range(cores):
        for k in range(lines):
            for x in range(peers):
                rows_ref[c, k, x] = rows[c * part : (c + 1) * part]


def turned(x):
    half = x.shape[1] // 2
    return jnp.concatenate([x[:, half:], x[:, :half]], axis=1)


def joined(left, right):
    return jnp.where(iota(left.shape, 1) < left.shape[1] // 2, left, right)


def ffn_kernel(x_ref, *refs):
    *weights, out_ref = refs
    peers, _, span = x_ref.shape
    width = peers * span
    half = peers // 2
    x = jnp.concatenate([x_ref[(k + half) % peers] for k in range(peers)], axis=1)
    gate = dot(x, jnp.concatenate([w[:width] for w in weights], axis=1))
    up = dot(x, jnp.concatenate([w[width : 2 * width] for w in weights], axis=1))
    hidden = (gate / (1.0 + jnp.exp(-gate)) * up).astype(BF)
    for k in range(half):
        tiles = []
        for block in (k, k + half):
            at = 2 * width + block * span
            tiles.append(jnp.concatenate([w[at : at + span] for w in weights], axis=0))
        both = dot(hidden, jnp.concatenate(tiles, axis=1))
        low, high = both[:, :span], both[:, span:]
        out_ref[k + half] = joined(low, turned(high)).astype(BF)
        out_ref[k] = joined(turned(low), high).astype(BF)


def expand_kernel(parts_ref, slots_ref, out_ref):
    cores, lines, peers, part, width = parts_ref.shape
    blocks, most, _ = slots_ref.shape
    slots = blocks * most
    halves = []
    for c in range(cores):
        total = jnp.zeros((part, width), F32)
        for k in range(lines):
            for x in range(peers):
                total = total + parts_ref[c, k, x].astype(F32)
        halves.append(total)
    rows = jnp.concatenate(halves, axis=0)
    rows = jnp.concatenate([rows, turned(rows)], axis=1).astype(BF)
    live = one_hot(slots_ref[...].reshape(slots, width).astype(F32) < LIMIT)
    in_block = one_hot(iota((blocks, slots), 0) == iota((blocks, slots), 1) // most)
    counts = dot(in_block, live).astype(BF)
    few = slots // 2
    step = most // 2
    block = iota((few, blocks), 0) // step
    before = dot(one_hot(iota((few, blocks), 1) < block), counts)
    count = dot(one_hot(iota((few, blocks), 1) == block), counts)
    lanes = iota((few, width), 1).astype(F32)
    found = []
    for half in range(2):
        place = (iota((few, width), 0) % step + half * step).astype(F32)
        rank = jnp.where(place < count, before + place, -1.0)
        put = [one_hot(rank - k == lanes) for k in range(0, cores * part, width)]
        found.append(dot(jnp.concatenate(put, axis=1), rows))
    first, second = found
    for g in range(2):
        straight, swapped = (slice(0, width), slice(width, 2 * width))
        if g == 0:
            out = joined(first[:, straight], second[:, swapped])
        else:
            out = joined(first[:, swapped], second[:, straight])
        out_ref[:, g] = out.astype(BF).reshape(blocks, step, width)


def combine_kernel(mix_ref, rows_ref, out_ref):
    layers, _, teams, step, width = rows_ref.shape
    both = [rows_ref[:, c].reshape(layers * teams * step, width) for c in (1, 0)]
    both = jnp.concatenate(both, axis=1)
    first = dot(mix_ref[0, 0], both) + dot(mix_ref[0, 1], both)
    second = dot(mix_ref[1, 0], both) + dot(mix_ref[1, 1], both)
    low = first[:, :width] + turned(second[:, :width])
    high = turned(first[:, width:]) + second[:, width:]
    out_ref[...] = joined(low, high).astype(BF)


def local_call(kernel, outs, *args, place=None, params=(), hbm=(), scratch=()):
    vmem = pl.BlockSpec(memory_space=pltpu.VMEM)
    specs = [pl.BlockSpec()] * len(params) + [vmem] * len(args)
    specs += [pl.BlockSpec(memory_space=pltpu.HBM)] * len(hbm)
    args = [pltpu.with_memory_space_constraint(a, pltpu.VMEM) for a in args]
    args = [*params, *args, *(pltpu.with_memory_space_constraint(a, pltpu.HBM) for a in hbm)]
    if place is not None:
        specs = [pl.BlockSpec(memory_space=pltpu.SMEM)] + specs
        args = [place] + args
    return pl.pallas_call(
        kernel,
        in_specs=specs,
        out_specs=jax.tree.map(
            lambda o: pl.BlockSpec(memory_space=getattr(o, "memory_space", None)), outs
        ),
        out_shape=outs,
        scratch_shapes=scratch,
        compiler_params=pltpu.CompilerParams(vmem_limit_bytes=24 * 2**20),
    )(*args)


def array(shape, dtype=BF):
    return pltpu.VMEM(shape, dtype)


def per_device(tokens, selected, affinity, w_gate, w_up, w_down):
    ep = lax.axis_size(EP)
    layers = lax.axis_size("z")
    team = lax.axis_size(TEAM)
    tok, width = tokens.shape
    experts, most = selected.shape
    span = width // team
    part = ep * most // 4
    lines = lax.axis_size("yy")
    peers = lax.axis_size("x")
    place = lax.axis_index(TP).astype(jnp.int32).reshape(1)
    packed = local_call(
        pack_kernel,
        array((3 * width, span)),
        hbm=(w_gate, w_up, w_down),
        scratch=[pltpu.SemaphoreType.DMA((2 + team,))],
    )
    mine = lax.ppermute(packed, ("c", "g", "yy"), TRADE)
    rows = local_call(
        pick_kernel,
        pltpu.HBM((layers, 2, most, span), BF),
        place=place,
        hbm=(selected, tokens),
        scratch=[
            pltpu.VMEM((experts, most), jnp.int32),
            pltpu.VMEM((2, tok, span), BF),
            pltpu.VMEM((2, layers, most, span), BF),
            pltpu.SemaphoreType.DMA((5,)),
        ],
    )
    arrived = lax.all_to_all(
        rows.reshape(ep, most, span),
        EP,
        0,
        0,
        axis_index_groups=turned_groups(layers, 1),
        tiled=True,
    )
    mix = local_call(
        mix_kernel,
        array((2, 2, tok, experts * most // 2)),
        params=(selected, affinity),
    )
    other = lax.ppermute(mine, "c", CORES)
    copies = local_call(compact_kernel, array((2, lines, peers, part, span)), arrived)
    chosen = lax.all_to_all(
        copies.reshape(team, part, span),
        TEAM,
        0,
        0,
        axis_index_groups=team_groups(team),
        tiled=True,
    )
    partial = local_call(
        ffn_kernel,
        array((team, part, span)),
        chosen,
        mine,
        other,
    )
    summands = lax.all_to_all(partial, TEAM, 0, 0, axis_index_groups=team_groups(team), tiled=True)
    result = local_call(
        expand_kernel,
        array((ep, 2, most // 2, span)),
        summands.reshape(2, lines, peers, part, span),
        arrived,
    )
    returned = lax.all_to_all(
        result.reshape(2 * ep, most // 2, span),
        ("z", "c", "g"),
        0,
        0,
        axis_index_groups=turned_groups(layers, 2),
        tiled=True,
    )
    return local_call(
        combine_kernel,
        jax.ShapeDtypeStruct((tok, span), BF),
        mix,
        returned.reshape(layers, 2, 2, most // 2, span),
    )


def solution(mesh):
    torus = Mesh(mesh.devices.reshape(16, 2, 2, 2, 4), ("z", "c", "g", "yy", "x"))
    in_specs = (
        P(EP, None),
        P(None, EP),
        P(None, EP),
        P(EP, None, TP),
        P(EP, None, TP),
        P(EP, TP, None),
    )

    return jax.shard_map(
        per_device, mesh=torus, in_specs=in_specs, out_specs=P(EP, TP), check_vma=False
    )
```

```python
import jax
import jax.numpy as jnp
from jax import lax
from jax.experimental import pallas as pl
from jax.experimental.pallas import tpu as pltpu
from jax.sharding import Mesh
from jax.sharding import PartitionSpec as P

EP = ("z", "c")
TP = ("g", "yy", "x")
TEAM = ("c", "yy", "x")
BF = jnp.bfloat16
F32 = jnp.float32
EMPTY = 64.0
LIMIT = 32.0
FIRST = 10
TRADE = [(0, 0), (1, 1), (6, 6), (7, 7), (4, 3), (3, 4), (5, 2), (2, 5)]
CORES = [(0, 1), (1, 0)]


def turned_groups(layers, teams):
    order = [(p + FIRST) % layers for p in range(layers)]
    return [[(z * 2 + c) * teams + g for z in order for c in (1, 0) for g in range(teams)]]


def team_groups(members):
    return [[(k + members // 2) % members for k in range(members)]]


def iota(shape, dim):
    return lax.broadcasted_iota(jnp.int32, shape, dim)


def dot(a, b):
    return jnp.dot(a, b, preferred_element_type=F32)


def one_hot(mask):
    return jnp.where(mask, 1.0, 0.0).astype(BF)


def pack_kernel(gate_ref, up_ref, down_ref, out_ref, rest_ref, down_out_ref, sems):
    _, width, span = gate_ref.shape
    copies = [(gate_ref.at[0], out_ref.at[:width]), (up_ref.at[0], out_ref.at[width:])]
    for at in range(0, width, span):
        copies.append((down_ref.at[0, :, at : at + span], down_out_ref.at[at : at + span]))
    copies = [pltpu.make_async_copy(*c, sems.at[k]) for k, c in enumerate(copies)]
    for copy in copies:
        copy.start()
    for copy in copies:
        copy.wait()
    store = pltpu.make_async_copy(down_out_ref, rest_ref, sems.at[0])
    store.start()
    store.wait()


def pick_kernel(place_ref, selected_ref, tokens_ref, rows_ref, sel_ref, tile_ref, out_ref, sems):
    g = place_ref[0] // 8
    experts, most = selected_ref.shape
    _, tok, width = tile_ref.shape
    first = pltpu.make_async_copy(selected_ref, sel_ref, sems.at[4])
    first.start()
    loads = []
    for c in range(2):
        at = pl.multiple_of((8 * (1 - c) + place_ref[0] % 8) * width, width)
        loads.append(
            pltpu.make_async_copy(tokens_ref.at[:, pl.ds(at, width)], tile_ref.at[c], sems.at[c])
        )
        loads[c].start()
    here = experts // 2
    slots = here * most
    first.wait()
    sel = sel_ref[...].astype(F32).astype(BF)
    layer = (iota((slots, experts), 0) // most + FIRST) % here
    repeat = one_hot(2 * layer + g == iota((slots, experts), 1))
    own = iota((slots, most), 0) % most == iota((slots, most), 1)
    spread = jnp.where(own, dot(repeat, sel), 0.0).astype(BF)
    position = dot(spread, jnp.ones((most, tok), BF))
    named = one_hot(position == iota((slots, tok), 1).astype(F32))
    stores = []
    for c in range(2):
        loads[c].wait()
        rows = jnp.where(position < 0.0, EMPTY, dot(named, tile_ref[c])).astype(BF)
        out_ref[c] = rows.reshape(here, most, width)
        stores.append(pltpu.make_async_copy(out_ref.at[c], rows_ref.at[:, c], sems.at[2 + c]))
        stores[c].start()
    for store in stores:
        store.wait()


def mix_kernel(selected_ref, affinity_ref, out_ref, mix_ref, sem):
    experts, most = selected_ref.shape
    _, _, tok, slots = mix_ref.shape
    part = most // 2
    expert = (iota((experts, slots), 1) // part + 2 * FIRST) % experts
    mine = iota((experts, slots), 0) == expert
    sel = selected_ref[...].astype(F32).astype(BF)
    aff = affinity_ref[...]
    high = aff.astype(BF)
    low = (aff - high.astype(F32)).astype(BF)
    for half in range(2):
        wanted = iota((most, slots), 1) % part + half * part
        tile = one_hot(iota((most, slots), 0) == wanted)

        def as_row(values):
            return jnp.sum(jnp.where(mine, dot(values, tile), 0.0), axis=0, keepdims=True)

        hit = as_row(sel) == iota((tok, slots), 0).astype(F32)
        mix_ref[half, 0] = jnp.where(hit, as_row(high), 0.0).astype(BF)
        mix_ref[half, 1] = jnp.where(hit, as_row(low), 0.0).astype(BF)
    store = pltpu.make_async_copy(mix_ref, out_ref, sem)
    store.start()
    store.wait()


def compact_kernel(slots_ref, rows_ref):
    blocks, most, width = slots_ref.shape
    cores, lines, peers, part, _ = rows_ref.shape
    slots = blocks * most
    count = cores * part
    data = slots_ref[...].reshape(slots, width)
    live = one_hot(data.astype(F32) < LIMIT)
    first = one_hot(iota((8, width), 1) == 0)
    live_row = lax.dot_general(first, live, (((1,), (1,)), ((), ())), preferred_element_type=F32)
    in_block = one_hot(iota((slots, blocks), 0) // most == iota((slots, blocks), 1))
    before = one_hot(iota((blocks, slots), 0) < iota((blocks, slots), 1) // most)
    counts = dot(live_row.astype(BF), in_block)
    rank = dot(counts.astype(BF), before) + (iota((8, slots), 1) % most).astype(F32)
    rank = jnp.where(live_row > 0.5, rank, -1.0)[0:1]
    take = one_hot(rank == iota((count, slots), 0).astype(F32))
    rows = dot(take, data).astype(BF)
    for c in range(cores):
        for k in range(lines):
            for x in range(peers):
                rows_ref[c, k, x] = rows[c * part : (c + 1) * part]


def turned(x):
    half = x.shape[1] // 2
    return jnp.concatenate([x[:, half:], x[:, :half]], axis=1)


def joined(left, right):
    return jnp.where(iota(left.shape, 1) < left.shape[1] // 2, left, right)


def ffn_kernel(x_ref, mine_ref, other_ref, mine_down_ref, other_down_ref, out_ref, down_ref, sems):
    peers, _, span = x_ref.shape
    width = peers * span
    loads = []
    for k, ref in enumerate((mine_down_ref, other_down_ref)):
        loads.append(pltpu.make_async_copy(ref, down_ref.at[k], sems.at[k]))
        loads[k].start()
    half = peers // 2
    x = jnp.concatenate([x_ref[(k + half) % peers] for k in range(peers)], axis=1)
    pair = (mine_ref, other_ref)
    gate = dot(x, jnp.concatenate([w[:width] for w in pair], axis=1))
    up = dot(x, jnp.concatenate([w[width:] for w in pair], axis=1))
    hidden = (gate / (1.0 + jnp.exp(-gate)) * up).astype(BF)
    for load in loads:
        load.wait()
    for k in range(half):
        tiles = []
        for at in (k * span, (k + half) * span):
            tiles.append(jnp.concatenate([down_ref[j, at : at + span] for j in range(2)], axis=0))
        both = dot(hidden, jnp.concatenate(tiles, axis=1))
        low, high = both[:, :span], both[:, span:]
        out_ref[k + half] = joined(low, turned(high)).astype(BF)
        out_ref[k] = joined(turned(low), high).astype(BF)


def expand_kernel(parts_ref, slots_ref, out_ref):
    cores, lines, peers, part, width = parts_ref.shape
    blocks, most, _ = slots_ref.shape
    slots = blocks * most
    halves = []
    for c in range(cores):
        total = jnp.zeros((part, width), F32)
        for k in range(lines):
            for x in range(peers):
                total = total + parts_ref[c, k, x].astype(F32)
        halves.append(total)
    rows = jnp.concatenate(halves, axis=0)
    rows = jnp.concatenate([rows, turned(rows)], axis=1).astype(BF)
    live = one_hot(slots_ref[...].reshape(slots, width).astype(F32) < LIMIT)
    in_block = one_hot(iota((blocks, slots), 0) == iota((blocks, slots), 1) // most)
    counts = dot(in_block, live).astype(BF)
    few = slots // 2
    step = most // 2
    block = iota((few, blocks), 0) // step
    before = dot(one_hot(iota((few, blocks), 1) < block), counts)
    count = dot(one_hot(iota((few, blocks), 1) == block), counts)
    lanes = iota((few, width), 1).astype(F32)
    found = []
    for half in range(2):
        place = (iota((few, width), 0) % step + half * step).astype(F32)
        rank = jnp.where(place < count, before + place, -1.0)
        put = [one_hot(rank - k == lanes) for k in range(0, cores * part, width)]
        found.append(dot(jnp.concatenate(put, axis=1), rows))
    first, second = found
    for g in range(2):
        straight, swapped = (slice(0, width), slice(width, 2 * width))
        if g == 0:
            out = joined(first[:, straight], second[:, swapped])
        else:
            out = joined(first[:, swapped], second[:, straight])
        out_ref[:, g] = out.astype(BF).reshape(blocks, step, width)


def combine_kernel(mix_ref, rows_ref, out_ref):
    layers, _, teams, step, width = rows_ref.shape
    both = [rows_ref[:, c].reshape(layers * teams * step, width) for c in (1, 0)]
    both = jnp.concatenate(both, axis=1)
    first = dot(mix_ref[0, 0], both) + dot(mix_ref[0, 1], both)
    second = dot(mix_ref[1, 0], both) + dot(mix_ref[1, 1], both)
    low = first[:, :width] + turned(second[:, :width])
    high = turned(first[:, width:]) + second[:, width:]
    out_ref[...] = joined(low, high).astype(BF)


def local_call(kernel, outs, *args, place=None, params=(), hbm=(), scratch=()):
    vmem = pl.BlockSpec(memory_space=pltpu.VMEM)
    specs = [pl.BlockSpec()] * len(params) + [vmem] * len(args)
    specs += [pl.BlockSpec(memory_space=pltpu.HBM)] * len(hbm)
    args = [pltpu.with_memory_space_constraint(a, pltpu.VMEM) for a in args]
    args = [*params, *args, *(pltpu.with_memory_space_constraint(a, pltpu.HBM) for a in hbm)]
    if place is not None:
        specs = [pl.BlockSpec(memory_space=pltpu.SMEM)] + specs
        args = [place] + args
    return pl.pallas_call(
        kernel,
        in_specs=specs,
        out_specs=jax.tree.map(
            lambda o: pl.BlockSpec(memory_space=getattr(o, "memory_space", None)), outs
        ),
        out_shape=outs,
        scratch_shapes=scratch,
        compiler_params=pltpu.CompilerParams(vmem_limit_bytes=24 * 2**20),
    )(*args)


def array(shape, dtype=BF):
    return pltpu.VMEM(shape, dtype)


def per_device(tokens, selected, affinity, w_gate, w_up, w_down):
    ep = lax.axis_size(EP)
    layers = lax.axis_size("z")
    team = lax.axis_size(TEAM)
    tok, width = tokens.shape
    experts, most = selected.shape
    span = width // team
    part = ep * most // 4
    lines = lax.axis_size("yy")
    peers = lax.axis_size("x")
    place = lax.axis_index(TP).astype(jnp.int32).reshape(1)
    packed, rest = local_call(
        pack_kernel,
        [array((2 * width, span)), pltpu.HBM((width, span), BF)],
        hbm=(w_gate, w_up, w_down),
        scratch=[pltpu.VMEM((width, span), BF), pltpu.SemaphoreType.DMA((2 + team,))],
    )
    mine = lax.ppermute(packed, ("c", "g", "yy"), TRADE)
    mine_down = lax.ppermute(rest, ("c", "g", "yy"), TRADE)
    rows = local_call(
        pick_kernel,
        pltpu.HBM((layers, 2, most, span), BF),
        place=place,
        hbm=(selected, tokens),
        scratch=[
            pltpu.VMEM((experts, most), jnp.int32),
            pltpu.VMEM((2, tok, span), BF),
            pltpu.VMEM((2, layers, most, span), BF),
            pltpu.SemaphoreType.DMA((5,)),
        ],
    )
    arrived = lax.all_to_all(
        rows.reshape(ep, most, span),
        EP,
        0,
        0,
        axis_index_groups=turned_groups(layers, 1),
        tiled=True,
    )
    mix = local_call(
        mix_kernel,
        pltpu.HBM((2, 2, tok, experts * most // 2), BF),
        params=(selected, affinity),
        scratch=[
            pltpu.VMEM((2, 2, tok, experts * most // 2), BF),
            pltpu.SemaphoreType.DMA(()),
        ],
    )
    other = lax.ppermute(mine, "c", CORES)
    other_down = lax.ppermute(mine_down, "c", CORES)
    copies = local_call(compact_kernel, array((2, lines, peers, part, span)), arrived)
    chosen = lax.all_to_all(
        copies.reshape(team, part, span),
        TEAM,
        0,
        0,
        axis_index_groups=team_groups(team),
        tiled=True,
    )
    partial = local_call(
        ffn_kernel,
        array((team, part, span)),
        chosen,
        mine,
        other,
        hbm=(mine_down, other_down),
        scratch=[pltpu.VMEM((2, width, span), BF), pltpu.SemaphoreType.DMA((2,))],
    )
    summands = lax.all_to_all(partial, TEAM, 0, 0, axis_index_groups=team_groups(team), tiled=True)
    result = local_call(
        expand_kernel,
        array((ep, 2, most // 2, span)),
        summands.reshape(2, lines, peers, part, span),
        arrived,
    )
    returned = lax.all_to_all(
        result.reshape(2 * ep, most // 2, span),
        ("z", "c", "g"),
        0,
        0,
        axis_index_groups=turned_groups(layers, 2),
        tiled=True,
    )
    return local_call(
        combine_kernel,
        jax.ShapeDtypeStruct((tok, span), BF),
        mix,
        returned.reshape(layers, 2, 2, most // 2, span),
    )


def solution(mesh):
    torus = Mesh(mesh.devices.reshape(16, 2, 2, 2, 4), ("z", "c", "g", "yy", "x"))
    in_specs = (
        P(EP, None),
        P(None, EP),
        P(None, EP),
        P(EP, None, TP),
        P(EP, None, TP),
        P(EP, TP, None),
    )

    return jax.shard_map(
        per_device, mesh=torus, in_specs=in_specs, out_specs=P(EP, TP), check_vma=False
    )
```

```python
import jax
import jax.numpy as jnp
from jax import lax
from jax.experimental import pallas as pl
from jax.experimental.pallas import tpu as pltpu
from jax.sharding import Mesh
from jax.sharding import PartitionSpec as P

EP = ("z", "c")
TP = ("g", "yy", "x")
TEAM = ("c", "yy", "x")
BF = jnp.bfloat16
F32 = jnp.float32
EMPTY = 64.0
LIMIT = 32.0
FIRST = 11
TRADE = [(0, 0), (1, 1), (6, 6), (7, 7), (4, 3), (3, 4), (5, 2), (2, 5)]
CORES = [(0, 1), (1, 0)]


def turned_groups(layers, teams):
    order = [(p + FIRST) % layers for p in range(layers)]
    return [[(z * 2 + c) * teams + g for z in order for c in (1, 0) for g in range(teams)]]


def team_groups(members):
    return [[(k + members // 2) % members for k in range(members)]]


def iota(shape, dim):
    return lax.broadcasted_iota(jnp.int32, shape, dim)


def dot(a, b):
    return jnp.dot(a, b, preferred_element_type=F32)


def one_hot(mask):
    return jnp.where(mask, 1.0, 0.0).astype(BF)


def pack_kernel(gate_ref, up_ref, down_ref, out_ref, sems):
    _, width, span = gate_ref.shape
    copies = [(gate_ref.at[0], out_ref.at[:width]), (up_ref.at[0], out_ref.at[width : 2 * width])]
    for k in range(width // span):
        at = 2 * width + k * span
        copies.append((down_ref.at[0, :, k * span : (k + 1) * span], out_ref.at[at : at + span]))
    copies = [pltpu.make_async_copy(*c, sems.at[k]) for k, c in enumerate(copies)]
    for copy in copies:
        copy.start()
    for copy in copies:
        copy.wait()


def pick_kernel(place_ref, selected_ref, tokens_ref, rows_ref, sel_ref, tile_ref, out_ref, sems):
    g = place_ref[0] // 8
    experts, most = selected_ref.shape
    _, tok, width = tile_ref.shape
    first = pltpu.make_async_copy(selected_ref, sel_ref, sems.at[4])
    first.start()
    loads = []
    for c in range(2):
        at = pl.multiple_of((8 * (1 - c) + place_ref[0] % 8) * width, width)
        loads.append(
            pltpu.make_async_copy(tokens_ref.at[:, pl.ds(at, width)], tile_ref.at[c], sems.at[c])
        )
        loads[c].start()
    here = experts // 2
    slots = here * most
    first.wait()
    sel = sel_ref[...].astype(F32).astype(BF)
    layer = (iota((slots, experts), 0) // most + FIRST) % here
    repeat = one_hot(2 * layer + g == iota((slots, experts), 1))
    own = iota((slots, most), 0) % most == iota((slots, most), 1)
    spread = jnp.where(own, dot(repeat, sel), 0.0).astype(BF)
    position = dot(spread, jnp.ones((most, tok), BF))
    named = one_hot(position == iota((slots, tok), 1).astype(F32))
    stores = []
    for c in range(2):
        loads[c].wait()
        rows = jnp.where(position < 0.0, EMPTY, dot(named, tile_ref[c])).astype(BF)
        out_ref[c] = rows.reshape(here, most, width)
        stores.append(pltpu.make_async_copy(out_ref.at[c], rows_ref.at[:, c], sems.at[2 + c]))
        stores[c].start()
    for store in stores:
        store.wait()


def mix_kernel(selected_ref, affinity_ref, mix_ref):
    experts, most = selected_ref.shape
    _, _, tok, slots = mix_ref.shape
    part = most // 2
    expert = (iota((experts, slots), 1) // part + 2 * FIRST) % experts
    mine = iota((experts, slots), 0) == expert
    sel = selected_ref[...].astype(F32).astype(BF)
    aff = affinity_ref[...]
    high = aff.astype(BF)
    low = (aff - high.astype(F32)).astype(BF)
    for half in range(2):
        wanted = iota((most, slots), 1) % part + half * part
        tile = one_hot(iota((most, slots), 0) == wanted)

        def as_row(values):
            return jnp.sum(jnp.where(mine, dot(values, tile), 0.0), axis=0, keepdims=True)

        hit = as_row(sel) == iota((tok, slots), 0).astype(F32)
        mix_ref[half, 0] = jnp.where(hit, as_row(high), 0.0).astype(BF)
        mix_ref[half, 1] = jnp.where(hit, as_row(low), 0.0).astype(BF)


def compact_kernel(slots_ref, rows_ref):
    blocks, most, width = slots_ref.shape
    cores, lines, peers, part, _ = rows_ref.shape
    slots = blocks * most
    count = cores * part
    data = slots_ref[...].reshape(slots, width)
    live = one_hot(data.astype(F32) < LIMIT)
    first = one_hot(iota((8, width), 1) == 0)
    live_row = lax.dot_general(first, live, (((1,), (1,)), ((), ())), preferred_element_type=F32)
    in_block = one_hot(iota((slots, blocks), 0) // most == iota((slots, blocks), 1))
    before = one_hot(iota((blocks, slots), 0) < iota((blocks, slots), 1) // most)
    counts = dot(live_row.astype(BF), in_block)
    rank = dot(counts.astype(BF), before) + (iota((8, slots), 1) % most).astype(F32)
    rank = jnp.where(live_row > 0.5, rank, -1.0)[0:1]
    take = one_hot(rank == iota((count, slots), 0).astype(F32))
    rows = dot(take, data).astype(BF)
    for c in range(cores):
        for k in range(lines):
            for x in range(peers):
                rows_ref[c, k, x] = rows[c * part : (c + 1) * part]


def turned(x):
    half = x.shape[1] // 2
    return jnp.concatenate([x[:, half:], x[:, :half]], axis=1)


def joined(left, right):
    return jnp.where(iota(left.shape, 1) < left.shape[1] // 2, left, right)


def ffn_kernel(x_ref, *refs):
    *weights, out_ref = refs
    peers, _, span = x_ref.shape
    width = peers * span
    half = peers // 2
    x = jnp.concatenate([x_ref[(k + half) % peers] for k in range(peers)], axis=1)
    gate = dot(x, jnp.concatenate([w[:width] for w in weights], axis=1))
    up = dot(x, jnp.concatenate([w[width : 2 * width] for w in weights], axis=1))
    hidden = (gate / (1.0 + jnp.exp(-gate)) * up).astype(BF)
    for k in range(half):
        tiles = []
        for block in (k, k + half):
            at = 2 * width + block * span
            tiles.append(jnp.concatenate([w[at : at + span] for w in weights], axis=0))
        both = dot(hidden, jnp.concatenate(tiles, axis=1))
        low, high = both[:, :span], both[:, span:]
        out_ref[k + half] = joined(low, turned(high)).astype(BF)
        out_ref[k] = joined(turned(low), high).astype(BF)


def expand_kernel(parts_ref, slots_ref, out_ref):
    cores, lines, peers, part, width = parts_ref.shape
    blocks, most, _ = slots_ref.shape
    slots = blocks * most
    halves = []
    for c in range(cores):
        total = jnp.zeros((part, width), F32)
        for k in range(lines):
            for x in range(peers):
                total = total + parts_ref[c, k, x].astype(F32)
        halves.append(total)
    rows = jnp.concatenate(halves, axis=0)
    rows = jnp.concatenate([rows, turned(rows)], axis=1).astype(BF)
    live = one_hot(slots_ref[...].reshape(slots, width).astype(F32) < LIMIT)
    in_block = one_hot(iota((blocks, slots), 0) == iota((blocks, slots), 1) // most)
    counts = dot(in_block, live).astype(BF)
    few = slots // 2
    step = most // 2
    block = iota((few, blocks), 0) // step
    before = dot(one_hot(iota((few, blocks), 1) < block), counts)
    count = dot(one_hot(iota((few, blocks), 1) == block), counts)
    lanes = iota((few, width), 1).astype(F32)
    found = []
    for half in range(2):
        place = (iota((few, width), 0) % step + half * step).astype(F32)
        rank = jnp.where(place < count, before + place, -1.0)
        put = [one_hot(rank - k == lanes) for k in range(0, cores * part, width)]
        found.append(dot(jnp.concatenate(put, axis=1), rows))
    first, second = found
    for g in range(2):
        straight, swapped = (slice(0, width), slice(width, 2 * width))
        if g == 0:
            out = joined(first[:, straight], second[:, swapped])
        else:
            out = joined(first[:, swapped], second[:, straight])
        out_ref[:, g] = out.astype(BF).reshape(blocks, step, width)


def combine_kernel(mix_ref, rows_ref, out_ref):
    layers, _, teams, step, width = rows_ref.shape
    both = [rows_ref[:, c].reshape(layers * teams * step, width) for c in (1, 0)]
    both = jnp.concatenate(both, axis=1)
    first = dot(mix_ref[0, 0], both) + dot(mix_ref[0, 1], both)
    second = dot(mix_ref[1, 0], both) + dot(mix_ref[1, 1], both)
    low = first[:, :width] + turned(second[:, :width])
    high = turned(first[:, width:]) + second[:, width:]
    out_ref[...] = joined(low, high).astype(BF)


def local_call(kernel, outs, *args, place=None, params=(), hbm=(), scratch=()):
    vmem = pl.BlockSpec(memory_space=pltpu.VMEM)
    specs = [pl.BlockSpec()] * len(params) + [vmem] * len(args)
    specs += [pl.BlockSpec(memory_space=pltpu.HBM)] * len(hbm)
    args = [pltpu.with_memory_space_constraint(a, pltpu.VMEM) for a in args]
    args = [*params, *args, *(pltpu.with_memory_space_constraint(a, pltpu.HBM) for a in hbm)]
    if place is not None:
        specs = [pl.BlockSpec(memory_space=pltpu.SMEM)] + specs
        args = [place] + args
    return pl.pallas_call(
        kernel,
        in_specs=specs,
        out_specs=jax.tree.map(
            lambda o: pl.BlockSpec(memory_space=getattr(o, "memory_space", None)), outs
        ),
        out_shape=outs,
        scratch_shapes=scratch,
        compiler_params=pltpu.CompilerParams(vmem_limit_bytes=24 * 2**20),
    )(*args)


def array(shape, dtype=BF):
    return pltpu.VMEM(shape, dtype)


def per_device(tokens, selected, affinity, w_gate, w_up, w_down):
    ep = lax.axis_size(EP)
    layers = lax.axis_size("z")
    team = lax.axis_size(TEAM)
    tok, width = tokens.shape
    experts, most = selected.shape
    span = width // team
    part = ep * most // 4
    lines = lax.axis_size("yy")
    peers = lax.axis_size("x")
    place = lax.axis_index(TP).astype(jnp.int32).reshape(1)
    packed = local_call(
        pack_kernel,
        array((3 * width, span)),
        hbm=(w_gate, w_up, w_down),
        scratch=[pltpu.SemaphoreType.DMA((2 + team,))],
    )
    mine = lax.ppermute(packed, ("c", "g", "yy"), TRADE)
    rows = local_call(
        pick_kernel,
        pltpu.HBM((layers, 2, most, span), BF),
        place=place,
        hbm=(selected, tokens),
        scratch=[
            pltpu.VMEM((experts, most), jnp.int32),
            pltpu.VMEM((2, tok, span), BF),
            pltpu.VMEM((2, layers, most, span), BF),
            pltpu.SemaphoreType.DMA((5,)),
        ],
    )
    arrived = lax.all_to_all(
        rows.reshape(ep, most, span),
        EP,
        0,
        0,
        axis_index_groups=turned_groups(layers, 1),
        tiled=True,
    )
    mix = local_call(
        mix_kernel,
        array((2, 2, tok, experts * most // 2)),
        params=(selected, affinity),
    )
    other = lax.ppermute(mine, "c", CORES)
    copies = local_call(compact_kernel, array((2, lines, peers, part, span)), arrived)
    chosen = lax.all_to_all(
        copies.reshape(team, part, span),
        TEAM,
        0,
        0,
        axis_index_groups=team_groups(team),
        tiled=True,
    )
    partial = local_call(
        ffn_kernel,
        array((team, part, span)),
        chosen,
        mine,
        other,
    )
    summands = lax.all_to_all(partial, TEAM, 0, 0, axis_index_groups=team_groups(team), tiled=True)
    result = local_call(
        expand_kernel,
        array((ep, 2, most // 2, span)),
        summands.reshape(2, lines, peers, part, span),
        arrived,
    )
    returned = lax.all_to_all(
        result.reshape(2 * ep, most // 2, span),
        ("z", "c", "g"),
        0,
        0,
        axis_index_groups=turned_groups(layers, 2),
        tiled=True,
    )
    return local_call(
        combine_kernel,
        jax.ShapeDtypeStruct((tok, span), BF),
        mix,
        returned.reshape(layers, 2, 2, most // 2, span),
    )


def solution(mesh):
    torus = Mesh(mesh.devices.reshape(16, 2, 2, 2, 4), ("z", "c", "g", "yy", "x"))
    in_specs = (
        P(EP, None),
        P(None, EP),
        P(None, EP),
        P(EP, None, TP),
        P(EP, None, TP),
        P(EP, TP, None),
    )

    return jax.shard_map(
        per_device, mesh=torus, in_specs=in_specs, out_specs=P(EP, TP), check_vma=False
    )
```
